256 devices in a mesh: sp: 32 (over z, y), tp: 8 (over x, core).
Axes of the slice: x: 4, y: 4, z: 8, core: 2. Of those that a mesh axis runs over, the one named last changes fastest.
Arguments:
- latent: bfloat16 [16384, 2048], P(('sp', 'tp')), may hold values from -6 to 6
- context: bfloat16 [512, 2048], P('sp'), may hold values from -6 to 6
- condition: float32 [2048], replicated, may hold values from -6 to 6
- context_condition: float32 [2048], replicated, may hold values from -6 to 6
- norm_gain: float32 [2048], replicated, may hold values from 0.1 to 1.9
- shift_weight: bfloat16 [2048, 2048], P('sp', 'tp'), may hold values from -0.21875 to 0.21875
- scale_weight: bfloat16 [2048, 2048], P('sp', 'tp'), may hold values from -0.21875 to 0.21875
- gate_weight: bfloat16 [2048, 2048], P('sp', 'tp'), may hold values from -0.21875 to 0.21875
- query_weight: bfloat16 [2048, 1024], P(None, 'tp'), may hold values from -1 to 1
- key_weight: bfloat16 [2048, 512], P(None, 'tp'), may hold values from -1 to 1
- value_weight: bfloat16 [2048, 512], P(None, 'tp'), may hold values from -0.125 to 0.125
- query_gain: float32 [64], replicated, may hold values from 0.1 to 7.8
- key_gain: float32 [64], replicated, may hold values from 0.1 to 7.8
- output_weight: bfloat16 [1024, 2048], replicated, may hold values from -1 to 1
Outputs:
- updated: bfloat16 [16384, 2048], P(('sp', 'tp'))
The draws below stay inside these ranges and needn't reach their ends.
All inputs are finite; a program needn't handle non-finite values.
Results may differ from the reference program's by a relative error of at most 0.012.
The reference program's roundings to bfloat16 on the way count: a program that leaves them out, or rounds other values in their place, can miss the bound.
Values may be sent and summed in bfloat16 or wider, within the bound.
A program may use at most 64 MiB of HBM per device.

```python
import math
import jax
import jax.numpy as jnp
from jax import lax

D = 2048
HQ = 16
KVH = 8
CHANNEL_SPAN = 64
GRID_W = 64
PREFIX_ITEMS = 512
HIDDEN_ITEMS = 16384


def query_base(key):
    return jax.random.truncated_normal(jax.random.fold_in(key, 101), -6.0, 6.0, (D, HQ * CHANNEL_SPAN), jnp.float32) * D ** (-0.5)


def draw_query_weight(key, part):
    return query_base(key).astype(jnp.bfloat16)


def draw_key_weight(key, part):
    fresh = jax.random.truncated_normal(jax.random.fold_in(key, 102), -6.0, 6.0, (D, KVH * CHANNEL_SPAN), jnp.float32) * D ** (-0.5)
    return fresh.astype(jnp.bfloat16)


def gain_draw(key, salt):
    return 3.0 * (1.0 + 0.18 * jax.random.truncated_normal(jax.random.fold_in(key, salt), -5.0, 5.0, (CHANNEL_SPAN,), jnp.float32))


def draw_query_gain(key, part):
    return gain_draw(key, 103)


def draw_key_gain(key, part):
    return gain_draw(key, 104)


def draw_output_weight(key, part):
    base = jax.random.truncated_normal(jax.random.fold_in(key, 105), -6.0, 6.0, (HQ * CHANNEL_SPAN, D), jnp.float32)
    return (base * (HQ * CHANNEL_SPAN) ** (-0.5)).astype(jnp.bfloat16)


def steps_of(own_key, dims, pieces, low, largest):
    loudness = 1.0
    for dim, parts in pieces:
        draws = jax.random.uniform(jax.random.fold_in(jax.random.fold_in(own_key, 6), dim), (parts,), jnp.float32, low / len(pieces), largest / len(pieces))
        loudness = loudness * jnp.repeat(jnp.exp(draws), dims[dim] // parts).reshape((-1,) + (1,) * (len(dims) - 1 - dim))
    return loudness


def scatter_about(key, extent, deviation, most, shards=(), kind=jnp.bfloat16):
    entries = deviation * jax.random.normal(key, extent, jnp.float32)
    if shards:
        entries = entries * steps_of(key, extent, shards, -0.22, 0.18)
    return jnp.clip(entries, -most, most).astype(kind)


def setup_inputs(seed: int = 0) -> dict:
    keys = jax.random.split(jax.random.key(seed), 15)
    latent = scatter_about(keys[0], (HIDDEN_ITEMS, D), 1.0, 6.0, ((0, 256),))
    context = scatter_about(keys[1], (PREFIX_ITEMS, D), 1.0, 6.0, ((0, 32),))
    condition = scatter_about(keys[2], (D,), 1.0, 6.0, (), jnp.float32)
    context_condition = scatter_about(keys[3], (D,), 1.0, 6.0, (), jnp.float32)
    norm_gain = jnp.clip(1.0 + 0.18 * jax.random.normal(keys[4], (D,), jnp.float32), 0.1, 1.9)
    shift_weight = scatter_about(keys[5], (D, D), (D // 3) ** -0.5, 0.21875, ((0, 32), (1, 8)))
    scale_weight = scatter_about(keys[6], (D, D), (D // 3) ** -0.5, 0.21875, ((0, 32), (1, 8)))
    gate_weight = scatter_about(keys[7], (D, D), (D // 3) ** -0.5, 0.21875, ((0, 32), (1, 8)))
    query_weight = draw_query_weight(jax.random.fold_in(keys[14], 71), 0)
    key_weight = draw_key_weight(jax.random.fold_in(keys[14], 71), 0)
    value_weight = scatter_about(keys[10], (D, KVH * CHANNEL_SPAN), D ** -0.5, 0.125, ((1, 8),))
    query_gain = draw_query_gain(jax.random.fold_in(keys[14], 71), 0)
    key_gain = draw_key_gain(jax.random.fold_in(keys[14], 71), 0)
    output_weight = draw_output_weight(jax.random.fold_in(keys[14], 71), 0)
    return {"latent": latent, "context": context, "condition": condition, "context_condition": context_condition, "norm_gain": norm_gain, "shift_weight": shift_weight, "scale_weight": scale_weight, "gate_weight": gate_weight, "query_weight": query_weight, "key_weight": key_weight, "value_weight": value_weight, "query_gain": query_gain, "key_gain": key_gain, "output_weight": output_weight}


epsilon = 1e-06
rope_base = 10000.0

def modulate(tok_rows, norm_gain, shift_row, scale_row):
    wide = tok_rows.astype(jnp.float32)
    normed = wide * lax.rsqrt(lax.optimization_barrier(jnp.mean(wide * wide, axis=-1, keepdims=True)) + epsilon)
    return (normed * norm_gain * (1.0 + scale_row) + shift_row).astype(jnp.bfloat16)

def headnorm(raw, gain, heads):
    field = raw.reshape(raw.shape[0], heads, -1)
    return field * lax.rsqrt(lax.optimization_barrier(jnp.mean(field * field, axis=-1, keepdims=True)) + epsilon) * gain

def rotate(field, places):
    count = field.shape[0]
    heads = field.shape[1]
    quarter = field.shape[2] // 4
    grid_row = (places // GRID_W).astype(jnp.float32)
    grid_col = (places % GRID_W).astype(jnp.float32)
    inverse = rope_base ** (-jnp.arange(quarter, dtype=jnp.float32) / quarter)
    angles = jnp.stack([grid_row[:, None] * inverse, grid_col[:, None] * inverse], axis=1)[:, None]
    cosine = jnp.cos(angles)
    sine = jnp.sin(angles)
    matcher_content_couples = field.reshape(count, heads, 2, 2, quarter)
    first = matcher_content_couples[:, :, :, 0]
    second = matcher_content_couples[:, :, :, 1]
    turned = jnp.stack([first * cosine - second * sine, second * cosine + first * sine], axis=3)
    return turned.reshape(count, heads, 4 * quarter)

def reference(latent, context, condition, context_condition, norm_gain, shift_weight, scale_weight, gate_weight, query_weight, key_weight, value_weight, query_gain, key_gain, output_weight):
    activated = jax.nn.silu(jnp.stack([condition, context_condition])).astype(jnp.bfloat16)
    shifts = jnp.dot(activated, shift_weight, preferred_element_type=jnp.float32)
    scales = jnp.dot(activated, scale_weight, preferred_element_type=jnp.float32)
    gates = jnp.dot(activated, gate_weight, preferred_element_type=jnp.float32)
    hidden = modulate(latent, norm_gain, shifts[0], scales[0])
    context_hidden = modulate(context, norm_gain, shifts[1], scales[1])
    places = jnp.arange(HIDDEN_ITEMS, dtype=jnp.int32)
    probe_entries = rotate(headnorm(jnp.dot(hidden, query_weight, preferred_element_type=jnp.float32), query_gain, HQ), places).astype(jnp.bfloat16)
    latent_keys = rotate(headnorm(jnp.dot(hidden, key_weight, preferred_element_type=jnp.float32), key_gain, KVH), places).astype(jnp.bfloat16)
    latent_values = jnp.dot(hidden, value_weight, preferred_element_type=jnp.float32).astype(jnp.bfloat16).reshape(HIDDEN_ITEMS, KVH, CHANNEL_SPAN)
    context_keys = headnorm(jnp.dot(context_hidden, key_weight, preferred_element_type=jnp.float32), key_gain, KVH).astype(jnp.bfloat16)
    context_values = jnp.dot(context_hidden, value_weight, preferred_element_type=jnp.float32).astype(jnp.bfloat16).reshape(PREFIX_ITEMS, KVH, CHANNEL_SPAN)
    matcher_pieces = jnp.concatenate([context_keys, latent_keys], axis=0).astype(jnp.float32)
    value_rows = jnp.concatenate([context_values, latent_values], axis=0).astype(jnp.float32)
    prefix_mapped = math.log(HIDDEN_ITEMS / (2.0 * PREFIX_ITEMS))
    similarity_offset = jnp.concatenate([jnp.full((PREFIX_ITEMS,), prefix_mapped, jnp.float32), jnp.zeros((HIDDEN_ITEMS,), jnp.float32)])
    group_size = HQ // KVH
    group_extent = math.gcd(HIDDEN_ITEMS, 256)
    grouped = probe_entries.reshape(HIDDEN_ITEMS // group_extent, group_extent, KVH, group_size, CHANNEL_SPAN)

    def one_block(probe_segment):
        similarity_matrix = jnp.einsum('dmvk,hmk->dmvh', probe_segment.astype(jnp.float32), matcher_pieces) * CHANNEL_SPAN ** (-0.5) + similarity_offset
        row_peak = lax.optimization_barrier(jnp.max(similarity_matrix, axis=-1, keepdims=True))
        shares = jnp.exp(similarity_matrix - row_peak)
        row_total = lax.optimization_barrier(jnp.sum(shares, axis=-1))
        rounded = lax.optimization_barrier(shares.astype(jnp.bfloat16)).astype(jnp.float32)
        weighted = jnp.einsum('qkgn,nkd->qkgd', rounded, value_rows)
        return (weighted / row_total[..., None]).astype(jnp.bfloat16)
    attended = lax.map(one_block, grouped).reshape(HIDDEN_ITEMS, HQ * CHANNEL_SPAN)
    projected = jnp.dot(attended, output_weight, preferred_element_type=jnp.float32)
    return (latent.astype(jnp.float32) + gates[0] * projected).astype(jnp.bfloat16)
```

```python
import functools
import math

import jax
import jax.numpy as jnp
from jax import lax
from jax.experimental import pallas as pl
from jax.experimental.pallas import tpu as pltpu
from jax.sharding import Mesh
from jax.sharding import PartitionSpec as P

F32 = jnp.float32
BF16 = jnp.bfloat16
MESH = pl.DeviceIdType.MESH
AXES = ("z", "y", "x", "c")
NZ, NY, NX, NC = 8, 4, 4, 2
NT = NX * NC
D = 2048
HEAD = 64
OWN = 64
TOK = OWN * NT
CTX = 16
COLS = 2 * TOK
GRID_W = 64
EPS = 1e-06
FIRST_SLOTS = 6
LOG2E = math.log2(math.e)


def remote(src, dst, send, recv, device):
    return pltpu.make_async_remote_copy(
        src_ref=src, dst_ref=dst, send_sem=send, recv_sem=recv, device_id=device, device_id_type=MESH
    )


def column(row):
    n = row.shape[1]
    same = lax.broadcasted_iota(jnp.int32, (n, n), 0) == lax.broadcasted_iota(jnp.int32, (n, n), 1)
    return jnp.sum(jnp.where(same, jnp.broadcast_to(row, (n, n)), 0.0), axis=1, keepdims=True)


def kernel(
    latent,
    context,
    condition,
    context_condition,
    norm_gain,
    shift_w,
    scale_w,
    gate_w,
    query_w,
    key_w,
    value_w,
    query_gain,
    key_gain,
    output_w,
    out,
    wmod,
    wcat,
    kw,
    vw,
    wo,
    mod1,
    mod2,
    mod3,
    vecs,
    lat,
    hid,
    tables,
    qraw,
    qhl,
    kv,
    kk,
    vt,
    ctx,
    ckk,
    cvt,
    m_ref,
    o_ref,
    s_ref,
    mx_ref,
    osend,
    lmsend,
    orecv,
    lmrecv,
    asend,
    arecv,
    local_sem,
    mod1_s,
    mod1_r,
    mod2_s,
    mod2_r,
    mod3_s,
    mod3_r,
    lx_s,
    lx_r,
    lf_s,
    lf_r,
    lc_s,
    lc_r,
    q_s,
    q_r,
    kv_s,
    kv_r,
    ctx_s,
    ctx_r,
    o_s,
    o_r,
    lm_s,
    lm_r,
    a_s,
    a_r,
):
    z, y, x, c = (lax.axis_index(a) for a in AXES)
    sp = z * NY + y
    tp = x * NC + c

    def at_z(d):
        return lax.rem(z + d + NZ, NZ)

    def at_y(d):
        return lax.rem(y + d + NY, NY)

    def at_x(d):
        return lax.rem(x + d + NX, NX)

    def tp_peer(d):
        t = lax.rem(tp + d, NT)
        return t, {"x": t // NC, "c": lax.rem(t, NC)}

    odd = lax.rem(sp, 2)
    half = pl.ds(pl.multiple_of(odd * 64, 64), 64)
    other_half = pl.ds(pl.multiple_of((1 - odd) * 64, 64), 64)
    loads = [
        pltpu.make_async_copy(shift_w, wmod.at[half, pl.ds(0, 256)], local_sem.at[0]),
        pltpu.make_async_copy(scale_w, wmod.at[half, pl.ds(256, 256)], local_sem.at[1]),
        pltpu.make_async_copy(gate_w, wmod.at[half, pl.ds(512, 256)], local_sem.at[2]),
        pltpu.make_async_copy(query_w, wcat.at[:, pl.ds(0, 128)], local_sem.at[3]),
        pltpu.make_async_copy(key_w, kw, local_sem.at[4]),
        pltpu.make_async_copy(value_w, vw, local_sem.at[5]),
        pltpu.make_async_copy(output_w, wo, local_sem.at[6]),
        pltpu.make_async_copy(latent, lat.at[tp], local_sem.at[7]),
    ]
    for load in loads:
        load.start()

    barrier = pltpu.get_barrier_semaphore()
    for d in range(1, NZ):
        pl.semaphore_signal(barrier, inc=1, device_id={"z": at_z(d)}, device_id_type=MESH)
    for d in range(1, NY):
        pl.semaphore_signal(barrier, inc=1, device_id={"y": at_y(d)}, device_id_type=MESH)
    for d in range(1, NT):
        pl.semaphore_signal(barrier, inc=1, device_id=tp_peer(d)[1], device_id_type=MESH)

    wmod[other_half, :] = jnp.zeros((64, 768), BF16)
    pair = pl.ds(pl.multiple_of((sp // 2) * 128, 128), 128)
    c0 = jnp.broadcast_to(condition[:, pair], (16, 128))
    c1 = jnp.broadcast_to(context_condition[:, pair], (16, 128))
    line = lax.broadcasted_iota(jnp.int32, (16, 128), 0)
    both = jnp.where(line == 0, c0, jnp.where(line == 1, c1, 0.0))
    activated = (both / (1.0 + jnp.exp(-both))).astype(BF16)
    for load in loads[:3]:
        load.wait()
    part = jnp.dot(activated, wmod[...], preferred_element_type=F32)
    rows = jnp.concatenate(
        [
            part[0:1, 0:256],
            part[0:1, 256:512],
            part[0:1, 512:768],
            part[1:2, 0:256],
            part[1:2, 256:512],
            jnp.zeros((3, 256), F32),
        ],
        axis=0,
    )
    mod1[z] = rows
    loads[7].wait()
    pl.semaphore_wait(barrier, NZ - 1 + NY - 1 + NT - 1)

    top, low = pl.ds(0, 32), pl.ds(32, 32)
    right, left = {"x": at_x(1)}, {"x": at_x(-1)}
    mate = {"c": 1 - c}

    def block_of(d):
        return at_x(d) * NC + c

    def lat_half(d, rows_):
        return lat.at[block_of(d), rows_]

    sends = []

    def go(copy):
        copy.start()
        sends.append(copy)

    go(remote(lat_half(0, top), lat_half(0, top), lx_s.at[0], lx_r.at[0], right))
    go(remote(lat_half(0, low), lat_half(0, low), lx_s.at[1], lx_r.at[1], left))
    for d in range(1, NZ):
        go(remote(mod1.at[z], mod1.at[z], mod1_s.at[d - 1], mod1_r.at[z], {"z": at_z(d)}))
    go(remote(lat_half(0, low), lat_half(0, low), lx_s.at[2], lx_r.at[2], right))
    go(remote(lat_half(0, top), lat_half(0, top), lx_s.at[3], lx_r.at[3], left))
    go(remote(lat.at[tp], lat.at[tp], lc_s.at[0], lc_r.at[0], mate))

    loads[3].wait()
    loads[4].wait()
    loads[5].wait()
    wcat[:, 128:256] = jnp.concatenate([kw[...], vw[...]], axis=1)
    lane = lax.broadcasted_iota(jnp.int32, (16, TOK), 1)
    freq = jnp.exp(
        lax.broadcasted_iota(jnp.int32, (16, TOK), 0).astype(F32) * (-math.log(10000.0) / 16.0)
    )
    row_angle = (lane // GRID_W + sp * (TOK // GRID_W)).astype(F32) * freq
    col_angle = lax.rem(lane, GRID_W).astype(F32) * freq
    tables[0] = jnp.cos(row_angle)
    tables[1] = jnp.sin(row_angle)
    tables[2] = jnp.cos(col_angle)
    tables[3] = jnp.sin(col_angle)
    for r in range(NZ):
        vt[r, 64:80, :] = jnp.ones((16, TOK), BF16)
    cvt[64:80, :] = jnp.ones((16, CTX * NZ), BF16)
    m_ref[...] = jnp.full(m_ref.shape, -1e30, F32)
    o_ref[...] = jnp.zeros(o_ref.shape, F32)

    def arrived(dst, sem):
        remote(dst, dst, lx_s.at[0], sem, mate).wait_recv()

    arrived(lat_half(-1, top), lx_r.at[0])
    go(remote(lat_half(-1, top), lat_half(-1, top), lf_s.at[0], lf_r.at[0], right))
    go(remote(lat_half(-1, top), lat_half(-1, top), lc_s.at[1], lc_r.at[1], mate))
    arrived(lat_half(1, low), lx_r.at[1])
    go(remote(lat_half(1, low), lat_half(1, low), lf_s.at[1], lf_r.at[1], left))
    go(remote(lat_half(1, low), lat_half(1, low), lc_s.at[2], lc_r.at[2], mate))

    for d in range(1, NZ):
        s = at_z(d)
        arrived(mod1.at[s], mod1_r.at[s])
    mod2[y] = jnp.sum(mod1[...], axis=0)
    for d in range(1, NY):
        go(remote(mod2.at[y], mod2.at[y], mod2_s.at[d - 1], mod2_r.at[y], {"y": at_y(d)}))

    arrived(lat_half(-1, low), lx_r.at[2])
    go(remote(lat_half(-1, low), lat_half(-1, low), lc_s.at[3], lc_r.at[3], mate))
    arrived(lat_half(1, top), lx_r.at[3])
    go(remote(lat_half(1, top), lat_half(1, top), lc_s.at[4], lc_r.at[4], mate))

    for d in range(1, NY):
        s = at_y(d)
        arrived(mod2.at[s], mod2_r.at[s])
    mod3[tp] = jnp.sum(mod2[...], axis=0)
    for d in range(1, NT):
        t, device = tp_peer(d)
        go(remote(mod3.at[tp], mod3.at[tp], mod3_s.at[d - 1], mod3_r.at[tp], device))

    arrived(lat_half(2, top), lf_r.at[0])
    go(remote(lat_half(2, top), lat_half(2, top), lc_s.at[5], lc_r.at[5], mate))
    arrived(lat_half(2, low), lf_r.at[1])
    go(remote(lat_half(2, low), lat_half(2, low), lc_s.at[6], lc_r.at[6], mate))

    for d in range(1, NT):
        t, device = tp_peer(d)
        arrived(mod3.at[t], mod3_r.at[t])
    vec = jnp.concatenate([mod3[t] for t in range(NT)], axis=1)
    vecs[0:1] = norm_gain[...] * (1.0 + vec[1:2])
    vecs[1:2] = vec[0:1]
    vecs[2:3] = vec[2:3]
    vecs[3:4] = norm_gain[...] * (1.0 + vec[4:5])
    vecs[4:5] = vec[3:4]

    def modulated(rows_, gain, shift):
        wide = rows_.astype(F32)
        mean = jnp.mean(wide * wide, axis=1, keepdims=True)
        return ((wide * lax.rsqrt(mean + EPS)) * gain + shift).astype(BF16)

    hid[TOK : TOK + CTX, :] = modulated(context[...], vecs[3:4], vecs[4:5])

    def mate_block(d):
        return at_x(d) * NC + 1 - c

    arrived(lat.at[mate_block(0)], lc_r.at[0])
    arrived(lat.at[mate_block(-1), top], lc_r.at[1])
    arrived(lat.at[mate_block(1), low], lc_r.at[2])
    arrived(lat.at[mate_block(-1), low], lc_r.at[3])
    arrived(lat.at[mate_block(1), top], lc_r.at[4])
    arrived(lat.at[mate_block(2), top], lc_r.at[5])
    arrived(lat.at[mate_block(2), low], lc_r.at[6])

    def normalize(i, carry):
        hid[pl.ds(pl.multiple_of(i * 32, 32), 32), :] = modulated(
            lat[i // 2, pl.ds(pl.multiple_of(lax.rem(i, 2) * 32, 32), 32)], vecs[0:1], vecs[1:2]
        )
        return carry

    lax.fori_loop(0, 2 * NT, normalize, 0)

    projected = jnp.dot(hid[...], wcat[...], preferred_element_type=F32)
    turned = projected[0:TOK].T

    def normed(field, gain):
        mean = jnp.mean(field * field, axis=0, keepdims=True)
        return field * lax.rsqrt(mean + EPS) * gain

    def rotated(field):
        cr, sr, cc, sc = tables[0], tables[1], tables[2], tables[3]
        a, b, e, f = field[0:16], field[16:32], field[32:48], field[48:64]
        return jnp.concatenate(
            [a * cr - b * sr, b * cr + a * sr, e * cc - f * sc, f * cc + e * sc], axis=0
        )

    keys = rotated(normed(turned[128:192], column(key_gain[...])))
    packed = jnp.concatenate([keys[:, 0:256], keys[:, 256:512]], axis=0).T
    kv[0, 0:256, :] = packed.astype(BF16)
    values = turned[192:256].astype(BF16)
    for i in range(4):
        kv[0, 256 + 64 * i : 320 + 64 * i, :] = values[:, 128 * i : 128 * (i + 1)]
    cp = projected[TOK : TOK + CTX]
    ck = cp[:, 128:192]
    ck = ck * lax.rsqrt(jnp.mean(ck * ck, axis=1, keepdims=True) + EPS) * key_gain[...]
    ctx[z] = jnp.concatenate([ck, cp[:, 192:256]], axis=1).astype(BF16)

    up, down = {"z": at_z(1)}, {"z": at_z(-1)}
    part_of = (pl.ds(0, 256), pl.ds(256, 256))

    def pass_on(slot, to, chunk, device):
        go(
            remote(
                kv.at[slot, part_of[chunk]],
                kv.at[to, part_of[chunk]],
                kv_s.at[to - 1, chunk],
                kv_r.at[to - 1, chunk],
                device,
            )
        )

    def kv_arrived(slot, chunk):
        dst = kv.at[slot, part_of[chunk]]
        remote(dst, dst, kv_s.at[0, 0], kv_r.at[slot - 1, chunk], up).wait_recv()

    pass_on(0, 1, 0, up)
    pass_on(0, 2, 1, down)
    pass_on(0, 1, 1, up)
    pass_on(0, 2, 0, down)
    for d in range(1, NZ):
        go(remote(ctx.at[z], ctx.at[z], ctx_s.at[d - 1], ctx_r.at[z], {"z": at_z(d)}))

    for h in range(2):
        q = rotated(normed(turned[64 * h : 64 * h + 64], column(query_gain[...])))
        qraw[0, :, TOK * h : TOK * (h + 1)] = q.astype(BF16)
    y_of = (None, {"y": at_y(1)}, {"y": at_y(-1)}, {"y": at_y(2)})
    there = (None, 2, 1, 3)
    for g in range(1, NY):
        go(remote(qraw.at[0], qraw.at[there[g]], q_s.at[g - 1], q_r.at[there[g] - 1], y_of[g]))

    def prepare_queries(g):
        q = qraw[g].astype(F32) * (LOG2E * HEAD ** (-0.5))
        high = q.astype(BF16)
        qhl[g, 0:64, :] = high
        qhl[g, 64:128, :] = (q - high.astype(F32)).astype(BF16)

    def prepare_keys(slot):
        packed_keys = kv[slot, 0:256, :]
        first, second = packed_keys[:, 0:64], packed_keys[:, 64:128]
        kk[slot, 0:256, :] = jnp.concatenate([first, first], axis=1)
        kk[slot, 256:512, :] = jnp.concatenate([second, second], axis=1)
        for i in range(4):
            vt[slot, 0:64, 128 * i : 128 * (i + 1)] = kv[slot, 256 + 64 * i : 320 + 64 * i, :]

    first_tiles = FIRST_SLOTS * NY
    late_slots = NZ - FIRST_SLOTS
    tiles = NZ * NY

    def tile_of(t):
        u = t - first_tiles
        early = t < first_tiles
        slot = jnp.where(early, t // NY, FIRST_SLOTS + lax.rem(u + tiles, late_slots))
        group = jnp.where(early, lax.rem(t, NY), NY - 1 - (u + tiles) // late_slots + tiles // late_slots)
        return slot, group

    def score(t, side):
        slot, group = tile_of(t)
        s = jnp.dot(kk[slot], qhl[group], preferred_element_type=F32)
        s_ref[side] = s
        mx_ref[side] = jnp.max(s, axis=0, keepdims=True)

    def absorb(t, side):
        slot, group = tile_of(t)
        old = m_ref[group]
        new = jnp.maximum(old, mx_ref[side])
        p = jnp.exp2(s_ref[side] - new).astype(BF16)
        m_ref[group] = new
        o_ref[group] = o_ref[group] * jnp.exp2(old - new) + jnp.dot(
            vt[slot], p, preferred_element_type=F32
        )

    def absorb_context(g):
        s = jnp.dot(ckk[...], qhl[g], preferred_element_type=F32) + math.log2(TOK / (2.0 * CTX))
        old = m_ref[g]
        new = jnp.maximum(old, jnp.max(s, axis=0, keepdims=True))
        p = jnp.exp2(s - new).astype(BF16)
        m_ref[g] = new
        o_ref[g] = o_ref[g] * jnp.exp2(old - new) + jnp.dot(
            cvt[...], p, preferred_element_type=F32
        )

    def send_out(g):
        osend[g - 1] = o_ref[g, 0:64, :].astype(BF16)
        lmsend[g - 1, 0:1, :] = o_ref[g, 64:65, :]
        lmsend[g - 1, 1:2, :] = m_ref[g]
        to = there[g] - 1
        remote(osend.at[g - 1], orecv.at[to], o_s.at[g - 1], o_r.at[to], y_of[g]).start()
        remote(lmsend.at[g - 1], lmrecv.at[to], lm_s.at[g - 1], lm_r.at[to], y_of[g]).start()

    prepare_keys(0)
    prepare_queries(0)
    score(0, 0)
    for slot, chunk in ((1, 0), (2, 1), (1, 1), (2, 0)):
        kv_arrived(slot, chunk)
        pass_on(slot, slot + 2, chunk, up if slot == 1 else down)
    prepare_keys(1)
    prepare_keys(2)
    for g in (1, 2):
        dst = qraw.at[g]
        remote(dst, dst, q_s.at[0], q_r.at[g - 1], up).wait_recv()
        prepare_queries(g)

    later = []

    def body(j, carry):
        @pl.when(j == 1)
        def _():
            dst = qraw.at[3]
            remote(dst, dst, q_s.at[0], q_r.at[2], up).wait_recv()
            prepare_queries(3)

        @pl.when(j == 4)
        def _():
            for slot, chunk in ((3, 0), (4, 1)):
                kv_arrived(slot, chunk)
                fwd(slot, chunk)

        @pl.when(j == 5)
        def _():
            for slot, chunk in ((3, 1), (4, 0)):
                kv_arrived(slot, chunk)
                fwd(slot, chunk)
            prepare_keys(3)
            prepare_keys(4)

        @pl.when(j == 8)
        def _():
            for slot, chunk in ((5, 0), (6, 1)):
                kv_arrived(slot, chunk)
                fwd(slot, chunk)

        @pl.when(j == 9)
        def _():
            for slot, chunk in ((5, 1), (6, 0)):
                kv_arrived(slot, chunk)
            prepare_keys(5)
            prepare_keys(6)

        @pl.when(j == 12)
        def _():
            kv_arrived(7, 0)
            kv_arrived(7, 1)
            prepare_keys(7)
            for d in range(1, NZ):
                s = at_z(d)
                arrived(ctx.at[s], ctx_r.at[s])
            every = ctx[...].reshape(NZ * CTX, 128)
            ckk[...] = jnp.concatenate([every[:, 0:64], every[:, 0:64]], axis=1)
            cvt[0:64, :] = every.astype(F32).T[64:128].astype(BF16)
            for g in range(NY):
                absorb_context(g)

        for k, g in ((13, 3), (14, 2), (15, 1)):
            pl.when(j == k)(functools.partial(send_out, g))

        for u in range(2):
            t = 2 * j + u
            score(jnp.minimum(t + 1, tiles - 1), (u + 1) % 2)
            absorb(t, u % 2)
        return carry

    def fwd(slot, chunk):
        to = min(slot + 2, 7)
        remote(
            kv.at[slot, part_of[chunk]],
            kv.at[to, part_of[chunk]],
            kv_s.at[to - 1, chunk],
            kv_r.at[to - 1, chunk],
            up if slot % 2 == 1 else down,
        ).start()
        later.append((slot, to, chunk))

    lax.fori_loop(0, tiles // 2, body, 0)

    top_m = m_ref[0]
    for i in range(NY - 1):
        dst = lmrecv.at[i]
        remote(dst, dst, lm_s.at[0], lm_r.at[i], up).wait_recv()
        top_m = jnp.maximum(top_m, lmrecv[i, 1:2, :])
    weight = jnp.exp2(m_ref[0] - top_m)
    total = o_ref[0, 64:65, :] * weight
    mixed = o_ref[0, 0:64, :] * weight
    for i in (2, 1, 0):
        dst = orecv.at[i]
        remote(dst, dst, o_s.at[0], o_r.at[i], up).wait_recv()
        weight = jnp.exp2(lmrecv[i, 1:2, :] - top_m)
        total = total + lmrecv[i, 0:1, :] * weight
        mixed = mixed + orecv[i].astype(F32) * weight
    mixed = mixed / total
    attended = jnp.concatenate([mixed[:, 0:TOK], mixed[:, TOK:COLS]], axis=0).T.astype(BF16)
    for t in range(NT):
        asend[t] = attended[OWN * t : OWN * (t + 1)]
    arecv[tp] = asend[tp]
    for d in range(1, NT):
        t, device = tp_peer(d)
        go(remote(asend.at[t], arecv.at[tp], a_s.at[d - 1], a_r.at[tp], device))
    loads[6].wait()
    for d in range(1, NT):
        t, device = tp_peer(d)
        arrived(arecv.at[t], a_r.at[t])
    heads = jnp.concatenate([arecv[t] for t in range(NT)], axis=1)
    for i in range(4):
        cols = slice(512 * i, 512 * (i + 1))
        branch = jnp.dot(heads, wo[:, cols], preferred_element_type=F32)
        out[:, cols] = (
            lat[tp, :, cols].astype(F32) + vecs[2:3, cols] * branch
        ).astype(BF16)

    for copy in sends:
        copy.wait_send()
    for slot, to, chunk in later:
        remote(
            kv.at[slot, part_of[chunk]],
            kv.at[to, part_of[chunk]],
            kv_s.at[to - 1, chunk],
            kv_r.at[to - 1, chunk],
            up,
        ).wait_send()
    for g in range(1, NY):
        remote(osend.at[g - 1], orecv.at[g - 1], o_s.at[g - 1], o_r.at[g - 1], up).wait_send()
        remote(lmsend.at[g - 1], lmrecv.at[g - 1], lm_s.at[g - 1], lm_r.at[g - 1], up).wait_send()


def on_device(
    latent,
    context,
    condition,
    context_condition,
    norm_gain,
    shift_weight,
    scale_weight,
    gate_weight,
    query_weight,
    key_weight,
    value_weight,
    query_gain,
    key_gain,
    output_weight,
):
    vmem, hbm = pl.BlockSpec(memory_space=pltpu.VMEM), pl.BlockSpec(memory_space=pl.ANY)
    dma, V = pltpu.SemaphoreType.DMA, pltpu.VMEM
    return pl.pallas_call(
        kernel,
        out_shape=jax.ShapeDtypeStruct((OWN, D), BF16),
        in_specs=[hbm, vmem, vmem, vmem, vmem] + [hbm] * 6 + [vmem, vmem, hbm],
        out_specs=vmem,
        scratch_shapes=[
            V((128, 768), BF16),
            V((D, 256), BF16),
            V((D, 64), BF16),
            V((D, 64), BF16),
            V((1024, D), BF16),
            V((NZ, 8, 256), F32),
            V((NY, 8, 256), F32),
            V((NT, 8, 256), F32),
            V((8, D), F32),
            V((NT, OWN, D), BF16),
            V((TOK + CTX, D), BF16),
            V((4, 16, TOK), F32),
            V((NY, HEAD, COLS), BF16),
            V((NY, 2 * HEAD, COLS), BF16),
            V((NZ, 512, 128), BF16),
            V((NZ, TOK, 128), BF16),
            V((NZ, 80, TOK), BF16),
            V((NZ, CTX, 128), BF16),
            V((NZ * CTX, 128), BF16),
            V((80, NZ * CTX), BF16),
            V((NY, 1, COLS), F32),
            V((NY, 80, COLS), F32),
            V((2, TOK, COLS), F32),
            V((2, 1, COLS), F32),
            V((NY - 1, HEAD, COLS), BF16),
            V((NY - 1, 8, COLS), F32),
            V((NY - 1, HEAD, COLS), BF16),
            V((NY - 1, 8, COLS), F32),
            V((NT, OWN, 128), BF16),
            V((NT, OWN, 128), BF16),
            dma((8,)),
            dma((NZ - 1,)),
            dma((NZ,)),
            dma((NY - 1,)),
            dma((NY,)),
            dma((NT - 1,)),
            dma((NT,)),
            dma((4,)),
            dma((4,)),
            dma((2,)),
            dma((2,)),
            dma((7,)),
            dma((7,)),
            dma((NY - 1,)),
            dma((NY - 1,)),
            dma((NZ - 1, 2)),
            dma((NZ - 1, 2)),
            dma((NZ - 1,)),
            dma((NZ,)),
            dma((NY - 1,)),
            dma((NY - 1,)),
            dma((NY - 1,)),
            dma((NY - 1,)),
            dma((NT - 1,)),
            dma((NT,)),
        ],
        compiler_params=pltpu.CompilerParams(
            collective_id=0, has_side_effects=True, vmem_limit_bytes=60 * 2**20
        ),
    )(
        latent,
        context,
        condition.reshape(1, D),
        context_condition.reshape(1, D),
        norm_gain.reshape(1, D),
        shift_weight,
        scale_weight,
        gate_weight,
        query_weight,
        key_weight,
        value_weight,
        query_gain.reshape(1, HEAD),
        key_gain.reshape(1, HEAD),
        output_weight,
    )


def solution(mesh):
    split = Mesh(mesh.devices.reshape(NZ, NY, NX, NC), AXES)
    seq, tp, everything = ("z", "y"), ("x", "c"), AXES
    return jax.shard_map(
        on_device,
        mesh=split,
        in_specs=(
            P(everything, None),
            P(seq, None),
            P(),
            P(),
            P(),
            P(seq, tp),
            P(seq, tp),
            P(seq, tp),
            P(None, tp),
            P(None, tp),
            P(None, tp),
            P(),
            P(),
            P(),
        ),
        out_specs=P(everything, None),
        check_vma=False,
    )
```

```python
import functools
import math

import jax
import jax.numpy as jnp
from jax import lax
from jax.experimental import pallas as pl
from jax.experimental.pallas import tpu as pltpu
from jax.sharding import Mesh
from jax.sharding import PartitionSpec as P

F32 = jnp.float32
BF16 = jnp.bfloat16
MESH = pl.DeviceIdType.MESH
AXES = ("z", "y", "x", "c")
NZ, NY, NX, NC = 8, 4, 4, 2
NT = NX * NC
D = 2048
HEAD = 64
OWN = 64
TOK = OWN * NT
QUARTER = TOK // NX
ORDER = (0, -1, 1, 2)
CTX = 16
COLS = 2 * TOK
GRID_W = 64
EPS = 1e-06
LOG2E = math.log2(math.e)


def remote(src, dst, send, recv, device):
    return pltpu.make_async_remote_copy(
        src_ref=src, dst_ref=dst, send_sem=send, recv_sem=recv, device_id=device, device_id_type=MESH
    )


def column(row):
    n = row.shape[1]
    same = lax.broadcasted_iota(jnp.int32, (n, n), 0) == lax.broadcasted_iota(jnp.int32, (n, n), 1)
    return jnp.sum(jnp.where(same, jnp.broadcast_to(row, (n, n)), 0.0), axis=1, keepdims=True)


def kernel(
    latent,
    context_in,
    condition_in,
    context_condition_in,
    norm_gain_in,
    shift_w,
    scale_w,
    gate_w,
    query_w,
    key_w,
    value_w,
    query_gain_in,
    key_gain_in,
    output_w,
    out,
    context,
    condition,
    context_condition,
    norm_gain,
    query_gain,
    key_gain,
    result,
    wmod,
    wcat,
    kvw,
    wo,
    mod1,
    mod2,
    mod3,
    vecs,
    lat,
    hid,
    tables,
    qraw,
    qhl,
    kv,
    kk,
    vt,
    ctx,
    ckk,
    cvt,
    m_ref,
    o_ref,
    s_ref,
    mx_ref,
    osend,
    lmsend,
    orecv,
    lmrecv,
    asend,
    arecv,
    local_sem,
    out_sem,
    mod1_s,
    mod1_r,
    mod2_s,
    mod2_r,
    mod3_s,
    mod3_r,
    lat_s,
    lx_r,
    lf_r,
    lc_r,
    q_s,
    q_r,
    kv_s,
    kv_r,
    ctx_s,
    ctx_r,
    o_s,
    o_r,
    lm_s,
    lm_r,
    a_s,
    a_r,
):
    z, y, x, c = (lax.axis_index(a) for a in AXES)
    sp = z * NY + y
    tp = x * NC + c

    def at_z(d):
        return lax.rem(z + d + NZ, NZ)

    def at_y(d):
        return lax.rem(y + d + NY, NY)

    def at_x(d):
        return lax.rem(x + d + NX, NX)

    def tp_peer(d):
        t = lax.rem(tp + d, NT)
        return t, {"x": t // NC, "c": lax.rem(t, NC)}

    odd = lax.rem(sp, 2)
    half = pl.ds(pl.multiple_of(odd * 64, 64), 64)
    other_half = pl.ds(pl.multiple_of((1 - odd) * 64, 64), 64)
    loads = [
        pltpu.make_async_copy(shift_w, wmod.at[half, pl.ds(0, 256)], local_sem.at[0]),
        pltpu.make_async_copy(scale_w, wmod.at[half, pl.ds(256, 256)], local_sem.at[1]),
        pltpu.make_async_copy(gate_w, wmod.at[half, pl.ds(512, 256)], local_sem.at[2]),
        pltpu.make_async_copy(query_w, wcat.at[:, pl.ds(0, 128)], local_sem.at[3]),
        pltpu.make_async_copy(key_w, kvw.at[pl.ds(0, 64)], local_sem.at[4]),
        pltpu.make_async_copy(value_w, kvw.at[pl.ds(64, 64)], local_sem.at[5]),
        pltpu.make_async_copy(output_w, wo, local_sem.at[6]),
        pltpu.make_async_copy(latent, lat.at[tp], local_sem.at[7]),
        pltpu.make_async_copy(condition_in, condition, local_sem.at[8]),
        pltpu.make_async_copy(context_condition_in, context_condition, local_sem.at[9]),
        pltpu.make_async_copy(context_in, context, local_sem.at[10]),
        pltpu.make_async_copy(norm_gain_in, norm_gain, local_sem.at[11]),
        pltpu.make_async_copy(query_gain_in, query_gain, local_sem.at[12]),
        pltpu.make_async_copy(key_gain_in, key_gain, local_sem.at[13]),
    ]
    for i in (8, 9, 0, 1, 2, 7, 3, 4, 5, 10, 11, 12, 13, 6):
        loads[i].start()

    barrier = pltpu.get_barrier_semaphore()
    for d in range(1, NZ):
        pl.semaphore_signal(barrier, inc=1, device_id={"z": at_z(d)}, device_id_type=MESH)
    for d in range(1, NY):
        pl.semaphore_signal(barrier, inc=1, device_id={"y": at_y(d)}, device_id_type=MESH)
    for d in range(1, NT):
        pl.semaphore_signal(barrier, inc=1, device_id=tp_peer(d)[1], device_id_type=MESH)

    wmod[other_half, :] = jnp.zeros((64, 768), BF16)
    pair = pl.ds(pl.multiple_of((sp // 2) * 128, 128), 128)
    loads[8].wait()
    loads[9].wait()
    c0 = jnp.broadcast_to(condition[:, pair], (16, 128))
    c1 = jnp.broadcast_to(context_condition[:, pair], (16, 128))
    line = lax.broadcasted_iota(jnp.int32, (16, 128), 0)
    both = jnp.where(line == 0, c0, jnp.where(line == 1, c1, 0.0))
    activated = (both / (1.0 + jnp.exp(-both))).astype(BF16)
    for load in loads[:3]:
        load.wait()
    part = jnp.dot(activated, wmod[...], preferred_element_type=F32)
    rows = jnp.concatenate(
        [
            part[0:1, 0:256],
            part[0:1, 256:512],
            part[0:1, 512:768],
            part[1:2, 0:256],
            part[1:2, 256:512],
            jnp.zeros((3, 256), F32),
        ],
        axis=0,
    )
    mod1[z] = rows
    loads[7].wait()
    pl.semaphore_wait(barrier, NZ - 1 + NY - 1 + NT - 1)

    top, low = pl.ds(0, 32), pl.ds(32, 32)
    right, left = {"x": at_x(1)}, {"x": at_x(-1)}
    mate = {"c": 1 - c}

    def block_of(d):
        return at_x(d) * NC + c

    def lat_half(d, rows_):
        return lat.at[block_of(d), rows_]

    def go(copy):
        copy.start()

    go(remote(lat_half(0, top), lat_half(0, top), lat_s, lx_r.at[0], right))
    go(remote(lat_half(0, low), lat_half(0, low), lat_s, lx_r.at[1], left))
    for d in range(1, NZ):
        go(remote(mod1.at[z], mod1.at[z], mod1_s, mod1_r, {"z": at_z(d)}))
    go(remote(lat_half(0, low), lat_half(0, low), lat_s, lx_r.at[2], right))
    go(remote(lat_half(0, top), lat_half(0, top), lat_s, lx_r.at[3], left))
    go(remote(lat.at[tp], lat.at[tp], lat_s, lc_r.at[0], mate))

    loads[3].wait()
    loads[4].wait()
    loads[5].wait()
    wcat[:, 128:256] = kvw[...].T
    for load in loads[10:]:
        load.wait()
    lane = lax.broadcasted_iota(jnp.int32, (16, TOK), 1)
    freq = jnp.exp(
        lax.broadcasted_iota(jnp.int32, (16, TOK), 0).astype(F32) * (-math.log(10000.0) / 16.0)
    )
    row_angle = (lane // GRID_W + sp * (TOK // GRID_W)).astype(F32) * freq
    col_angle = lax.rem(lane, GRID_W).astype(F32) * freq
    tables[0] = jnp.cos(row_angle)
    tables[1] = jnp.sin(row_angle)
    tables[2] = jnp.cos(col_angle)
    tables[3] = jnp.sin(col_angle)
    for r in range(NZ):
        vt[r, 64:80, :] = jnp.ones((16, TOK), BF16)
    key_column, query_column = column(key_gain[...]), column(query_gain[...])
    cvt[64:80, :] = jnp.ones((16, CTX * NZ), BF16)
    m_ref[...] = jnp.full(m_ref.shape, -1e30, F32)
    o_ref[...] = jnp.zeros(o_ref.shape, F32)

    def arrived(dst, sem):
        remote(dst, dst, lat_s, sem, mate).wait_recv()

    arrived(mod1.at[pl.ds(0, NZ - 1)], mod1_r)
    mod2[y] = jnp.sum(mod1[...], axis=0)
    for d in range(1, NY):
        go(remote(mod2.at[y], mod2.at[y], mod2_s, mod2_r, {"y": at_y(d)}))

    piece = [pl.ds(16 * i, 16) for i in range(4)]

    def relay(d, i, device):
        go(remote(lat_half(d, piece[i]), lat_half(d, piece[i]), lat_s, lf_r.at[i], device))

    arrived(lat_half(-1, top), lx_r.at[0])
    relay(-1, 0, right)
    go(remote(lat_half(-1, top), lat_half(-1, top), lat_s, lc_r.at[1], mate))
    arrived(lat_half(1, low), lx_r.at[1])
    relay(1, 2, left)
    go(remote(lat_half(1, low), lat_half(1, low), lat_s, lc_r.at[2], mate))

    arrived(mod2.at[pl.ds(0, NY - 1)], mod2_r)
    mod3[tp] = jnp.sum(mod2[...], axis=0)
    for d in range(1, NT):
        t, device = tp_peer(d)
        go(remote(mod3.at[tp], mod3.at[tp], mod3_s, mod3_r, device))
    relay(-1, 1, right)
    relay(1, 3, left)

    arrived(lat_half(-1, low), lx_r.at[2])
    go(remote(lat_half(-1, low), lat_half(-1, low), lat_s, lc_r.at[3], mate))
    arrived(lat_half(1, top), lx_r.at[3])
    go(remote(lat_half(1, top), lat_half(1, top), lat_s, lc_r.at[4], mate))

    arrived(mod3.at[pl.ds(0, NT - 1)], mod3_r)
    vec = jnp.concatenate([mod3[t] for t in range(NT)], axis=1)
    vecs[0:1] = norm_gain[...] * (1.0 + vec[1:2])
    vecs[1:2] = vec[0:1]
    vecs[2:3] = vec[2:3]
    vecs[3:4] = norm_gain[...] * (1.0 + vec[4:5])
    vecs[4:5] = vec[3:4]

    def modulated(rows_, gain, shift):
        wide = rows_.astype(F32)
        mean = jnp.mean(wide * wide, axis=1, keepdims=True)
        return ((wide * lax.rsqrt(mean + EPS)) * gain + shift).astype(BF16)

    hid[QUARTER:, :] = modulated(context[...], vecs[3:4], vecs[4:5])

    def normed(field, gain):
        mean = jnp.mean(field * field, axis=0, keepdims=True)
        return field * lax.rsqrt(mean + EPS) * gain

    up, down = {"z": at_z(1)}, {"z": at_z(-1)}
    y_of = (None, {"y": at_y(1)}, {"y": at_y(-1)}, {"y": at_y(2)})
    there = (None, 2, 1, 3)

    def part_of(i):
        return pl.ds(pl.multiple_of(at_x(ORDER[i]) * QUARTER, QUARTER), QUARTER)

    def kv_copy(slot, to, i):
        return remote(
            kv.at[slot, part_of(i)],
            kv.at[to, part_of(i)],
            kv_s,
            kv_r.at[to - 1, i],
            down if to in (2, 4, 6) or slot == 6 else up,
        )

    def kv_arrived(slot, i):
        dst = kv.at[slot, part_of(i)]
        remote(dst, dst, kv_s, kv_r.at[slot - 1, i], up).wait_recv()

    def process(i):
        xb = at_x(ORDER[i])

        def normalize(k, carry):
            hid[pl.ds(pl.multiple_of(k * 32, 32), 32), :] = modulated(
                lat[xb * NC + k // 2, pl.ds(pl.multiple_of(lax.rem(k, 2) * 32, 32), 32)],
                vecs[0:1],
                vecs[1:2],
            )
            return carry

        lax.fori_loop(0, QUARTER // 32, normalize, 0)
        many = QUARTER + CTX if i == 0 else QUARTER
        projected = jnp.dot(hid[0:many], wcat[...], preferred_element_type=F32)
        turned = projected[0:QUARTER].T
        lanes = pl.ds(pl.multiple_of(xb * QUARTER, QUARTER), QUARTER)
        cr, sr, cc, sc = (tables[k, :, lanes] for k in range(4))

        def rotated(field):
            a, b, e, f = field[0:16], field[16:32], field[32:48], field[48:64]
            return jnp.concatenate(
                [a * cr - b * sr, b * cr + a * sr, e * cc - f * sc, f * cc + e * sc], axis=0
            )

        keys = rotated(normed(turned[128:192], key_column))
        packed = jnp.concatenate([keys[:, 0:64], keys[:, 64:128]], axis=0).T
        first = pl.multiple_of(xb * QUARTER, QUARTER)
        kv[0, pl.ds(first, 64), :] = packed.astype(BF16)
        kv[0, pl.ds(first + 64, 64), :] = turned[192:256].astype(BF16)
        go(kv_copy(0, 1, i))
        go(kv_copy(0, 2, i))
        for h in range(2):
            q = rotated(normed(turned[64 * h : 64 * h + 64], query_column))
            qraw[0, xb, :, QUARTER * h : QUARTER * (h + 1)] = q.astype(BF16)
        for g in range(1, NY):
            go(
                remote(
                    qraw.at[0, xb],
                    qraw.at[there[g], xb],
                    q_s,
                    q_r.at[there[g] - 1],
                    y_of[g],
                )
            )
        if i == 0:
            cp = projected[QUARTER : QUARTER + CTX]
            ck = cp[:, 128:192]
            ck = ck * lax.rsqrt(jnp.mean(ck * ck, axis=1, keepdims=True) + EPS) * key_gain[...]
            ctx[z] = jnp.concatenate([ck, cp[:, 192:256]], axis=1).astype(BF16)
            for d in range(1, NZ):
                go(remote(ctx.at[z], ctx.at[z], ctx_s, ctx_r, {"z": at_z(d)}))

    def mate_block(d):
        return at_x(d) * NC + 1 - c

    arrived(lat.at[mate_block(0)], lc_r.at[0])
    process(0)

    arrived(lat_half(2, piece[0]), lf_r.at[0])
    arrived(lat_half(2, piece[1]), lf_r.at[1])
    go(remote(lat_half(2, top), lat_half(2, top), lat_s, lc_r.at[5], mate))
    arrived(lat_half(2, piece[2]), lf_r.at[2])
    arrived(lat_half(2, piece[3]), lf_r.at[3])
    go(remote(lat_half(2, low), lat_half(2, low), lat_s, lc_r.at[6], mate))

    arrived(lat.at[mate_block(-1), top], lc_r.at[1])
    arrived(lat.at[mate_block(-1), low], lc_r.at[3])
    process(1)

    arrived(lat.at[mate_block(1), low], lc_r.at[2])
    arrived(lat.at[mate_block(1), top], lc_r.at[4])
    process(2)

    arrived(lat.at[mate_block(2), top], lc_r.at[5])
    arrived(lat.at[mate_block(2), low], lc_r.at[6])

    process(3)

    def prepare_queries(g):
        for k in range(NX):
            q = qraw[g, k].astype(F32) * (LOG2E * HEAD ** (-0.5))
            high = q.astype(BF16)
            cols = slice(2 * QUARTER * k, 2 * QUARTER * (k + 1))
            qhl[g, 0:64, cols] = high
            qhl[g, 64:128, cols] = (q - high.astype(F32)).astype(BF16)

    def prepare_keys(slot):
        for k in range(NX):
            first = QUARTER * k
            packed_keys = kv[slot, first : first + 64, :]
            low_lanes, high_lanes = packed_keys[:, 0:64], packed_keys[:, 64:128]
            kk[slot, first : first + 64, :] = jnp.concatenate([low_lanes, low_lanes], axis=1)
            kk[slot, first + 64 : first + 128, :] = jnp.concatenate([high_lanes, high_lanes], axis=1)
            vt[slot, 0:64, first : first + QUARTER] = kv[slot, first + 64 : first + QUARTER, :]

    tiles = NZ * NY

    def pick(cases, default):
        for test, value in reversed(cases):
            default = jnp.where(test, value, default)
        return default

    def tile_of(t):
        w, v = t - 1 + 6, t - 19 + 20
        slot = pick(
            [(t < 1, 0), (t < 5, w // 2 - 3), (t < 7, t - 5), (t < 19, w // 3 - 2), (t < 25, 6 + lax.rem(v, 2))],
            t - 24,
        )
        group = pick(
            [(t < 1, 0), (t < 5, 1 + lax.rem(w, 2)), (t < 7, 3), (t < 19, 1 + lax.rem(w, 3)), (t < 25, 13 - v // 2)],
            0,
        )
        return slot, group

    strips = [pl.ds(256 * k, 256) for k in range(COLS // 256)]

    def score_strip(tile, side, cols):
        slot, group = tile
        s = jnp.dot(kk[slot], qhl[group, :, cols], preferred_element_type=F32)
        s_ref[side, :, cols] = s
        mx_ref[side, :, cols] = jnp.max(s, axis=0, keepdims=True)

    def absorb_strip(tile, side, cols):
        slot, group = tile
        old = m_ref[group, :, cols]
        new = jnp.maximum(old, mx_ref[side, :, cols])
        p = jnp.exp2(s_ref[side, :, cols] - new).astype(BF16)
        m_ref[group, :, cols] = new
        o_ref[group, :, cols] = o_ref[group, :, cols] * jnp.exp2(old - new) + jnp.dot(
            vt[slot], p, preferred_element_type=F32
        )

    def score(t, side):
        for cols in strips:
            score_strip(tile_of(t), side, cols)

    def absorb(t, side):
        for cols in strips:
            absorb_strip(tile_of(t), side, cols)

    def absorb_context(g):
        s = jnp.dot(ckk[...], qhl[g], preferred_element_type=F32) + math.log2(TOK / (2.0 * CTX))
        old = m_ref[g]
        new = jnp.maximum(old, jnp.max(s, axis=0, keepdims=True))
        p = jnp.exp2(s - new).astype(BF16)
        m_ref[g] = new
        o_ref[g] = o_ref[g] * jnp.exp2(old - new) + jnp.dot(
            cvt[...], p, preferred_element_type=F32
        )

    def send_out(g):
        osend[g - 1] = o_ref[g, 0:64, :].astype(BF16)
        for i in range(4):
            lmsend[g - 1, i : i + 1, :] = o_ref[g, 64:65, 256 * i : 256 * (i + 1)]
            lmsend[g - 1, 4 + i : 5 + i, :] = m_ref[g, :, 256 * i : 256 * (i + 1)]
        to = there[g] - 1
        remote(osend.at[g - 1], orecv.at[to], o_s, o_r, y_of[g]).start()
        remote(lmsend.at[g - 1], lmrecv.at[to], lm_s, lm_r, y_of[g]).start()

    def pass_on(i):
        for slot in (1, 2):
            kv_arrived(slot, i)
            go(kv_copy(slot, slot + 2, i))

    prepare_keys(0)
    prepare_queries(0)
    pass_on(0)
    score(0, 0)
    absorb(0, 0)

    pass_on(1)
    pass_on(2)
    pass_on(3)
    prepare_keys(1)
    prepare_keys(2)

    def queries_arrived(g):
        remote(qraw.at[g], qraw.at[g], q_s, q_r.at[g - 1], up).wait_recv()
        prepare_queries(g)

    queries_arrived(1)
    queries_arrived(2)
    score(1, 1)

    def body(j, carry):
        @pl.when(j == 1)
        def _():
            queries_arrived(3)

        @pl.when(j == 1)
        def _():
            for slot in (3, 4):
                kv_arrived(slot, 0)
                fwd(slot, 0)

        @pl.when(j == 2)
        def _():
            for i in (1, 2):
                for slot in (3, 4):
                    kv_arrived(slot, i)
                    fwd(slot, i)

        @pl.when(j == 3)
        def _():
            for slot in (3, 4):
                kv_arrived(slot, 3)
                fwd(slot, 3)
            prepare_keys(3)
            prepare_keys(4)

        @pl.when(j == 5)
        def _():
            for i in (0, 1):
                kv_arrived(5, i)
                fwd(5, i)
                kv_arrived(6, i)

        @pl.when(j == 6)
        def _():
            for i in (2, 3):
                kv_arrived(6, i)
                fwd(6, i)
                kv_arrived(5, i)
            prepare_keys(5)
            prepare_keys(6)

        @pl.when(j == 9)
        def _():
            for i in range(NX):
                kv_arrived(7, i)
            prepare_keys(7)
            arrived(ctx.at[pl.ds(0, NZ - 1)], ctx_r)
            every = ctx[...].reshape(NZ * CTX, 128)
            ckk[...] = jnp.concatenate([every[:, 0:64], every[:, 0:64]], axis=1)
            cvt[0:64, :] = every.astype(F32).T[64:128].astype(BF16)
            for g in range(NY):
                absorb_context(g)

        for k, g in ((10, 3), (11, 2), (12, 1)):
            pl.when(j == k)(functools.partial(send_out, g))

        now = tile_of(2 * j + 1)
        for u in range(2):
            t = 2 * j + 1 + u
            side = (u + 1) % 2
            following = tile_of(t + 1)
            for cols in strips:
                score_strip(following, 1 - side, cols)
                absorb_strip(now, side, cols)
            now = following
        return carry

    def fwd(slot, i):
        copy = kv_copy(slot, min(slot + 2, 7), i)
        copy.start()

    lax.fori_loop(0, tiles // 2 - 1, body, 0)
    absorb(tiles - 1, 1)

    def unpacked(i, first):
        return jnp.concatenate([lmrecv[i, first + k : first + k + 1, :] for k in range(4)], axis=1)

    top_m = m_ref[0]
    remote(lmrecv, lmrecv, lm_s, lm_r, up).wait_recv()
    for i in range(NY - 1):
        top_m = jnp.maximum(top_m, unpacked(i, 4))
    weight = jnp.exp2(m_ref[0] - top_m)
    total = o_ref[0, 64:65, :] * weight
    mixed = o_ref[0, 0:64, :] * weight
    remote(orecv, orecv, o_s, o_r, up).wait_recv()
    for i in (2, 1, 0):
        weight = jnp.exp2(unpacked(i, 4) - top_m)
        total = total + unpacked(i, 0) * weight
        mixed = mixed + orecv[i].astype(F32) * weight
    mixed = mixed / total
    for k in range(NX):
        cols = mixed[:, 2 * QUARTER * k : 2 * QUARTER * (k + 1)]
        attended = jnp.concatenate([cols[:, 0:QUARTER], cols[:, QUARTER:]], axis=0).T.astype(BF16)
        for h in range(NC):
            asend[NC * k + h] = attended[OWN * h : OWN * (h + 1)]
    arecv[tp] = asend[tp]
    for d in range(1, NT):
        t, device = tp_peer(d)
        go(remote(asend.at[t], arecv.at[tp], a_s, a_r, device))
    loads[6].wait()
    arrived(arecv.at[pl.ds(0, NT - 1)], a_r)
    heads = jnp.concatenate([arecv[t] for t in range(NT)], axis=1)
    writes = []
    for i in range(4):
        cols = slice(512 * i, 512 * (i + 1))
        branch = jnp.dot(heads, wo[:, cols], preferred_element_type=F32)
        result[:, cols] = (
            lat[tp, :, cols].astype(F32) + vecs[2:3, cols] * branch
        ).astype(BF16)
        strip = pl.ds(512 * i, 512)
        write = pltpu.make_async_copy(result.at[:, strip], out.at[:, strip], out_sem.at[i])
        write.start()
        writes.append(write)

    for ref, sem in (
        (mod1.at[pl.ds(0, NZ - 1)], mod1_s),
        (mod2.at[pl.ds(0, NY - 1)], mod2_s),
        (mod3.at[pl.ds(0, NT - 1)], mod3_s),
        (lat.at[pl.ds(0, NT - 1)], lat_s),
        (qraw.at[pl.ds(0, NY - 1)], q_s),
        (kv.at[pl.ds(0, NZ - 1)], kv_s),
        (ctx.at[pl.ds(0, NZ - 1)], ctx_s),
        (osend, o_s),
        (lmsend, lm_s),
        (arecv.at[pl.ds(0, NT - 1)], a_s),
    ):
        remote(ref, ref, sem, sem, up).wait_send()
    for write in writes:
        write.wait()


def on_device(
    latent,
    context,
    condition,
    context_condition,
    norm_gain,
    shift_weight,
    scale_weight,
    gate_weight,
    query_weight,
    key_weight,
    value_weight,
    query_gain,
    key_gain,
    output_weight,
):
    hbm = pl.BlockSpec(memory_space=pl.ANY)
    dma, V = pltpu.SemaphoreType.DMA, pltpu.VMEM
    return pl.pallas_call(
        kernel,
        out_shape=jax.ShapeDtypeStruct((OWN, D), BF16),
        in_specs=[hbm] * 14,
        out_specs=hbm,
        scratch_shapes=[
            V((CTX, D), BF16),
            V((1, D), F32),
            V((1, D), F32),
            V((1, D), F32),
            V((1, HEAD), F32),
            V((1, HEAD), F32),
            V((OWN, D), BF16),
            V((128, 768), BF16),
            V((D, 256), BF16),
            V((128, D), BF16),
            V((1024, D), BF16),
            V((NZ, 8, 256), F32),
            V((NY, 8, 256), F32),
            V((NT, 8, 256), F32),
            V((8, D), F32),
            V((NT, OWN, D), BF16),
            V((QUARTER + CTX, D), BF16),
            V((4, 16, TOK), F32),
            V((NY, NX, HEAD, 2 * QUARTER), BF16),
            V((NY, 2 * HEAD, COLS), BF16),
            V((NZ, 512, 128), BF16),
            V((NZ, TOK, 128), BF16),
            V((NZ, 80, TOK), BF16),
            V((NZ, CTX, 128), BF16),
            V((NZ * CTX, 128), BF16),
            V((80, NZ * CTX), BF16),
            V((NY, 1, COLS), F32),
            V((NY, 80, COLS), F32),
            V((2, TOK, COLS), F32),
            V((2, 1, COLS), F32),
            V((NY - 1, HEAD, COLS), BF16),
            V((NY - 1, 8, 256), F32),
            V((NY - 1, HEAD, COLS), BF16),
            V((NY - 1, 8, 256), F32),
            V((NT, OWN, 128), BF16),
            V((NT, OWN, 128), BF16),
            dma((14,)),
            dma((4,)),
            dma,
            dma,
            dma,
            dma,
            dma,
            dma,
            dma,
            dma((4,)),
            dma((4,)),
            dma((7,)),
            dma,
            dma((NY - 1,)),
            dma,
            dma((NZ - 1, NX)),
            dma,
            dma,
            dma,
            dma,
            dma,
            dma,
            dma,
            dma,
        ],
        compiler_params=pltpu.CompilerParams(
            collective_id=0, has_side_effects=True, vmem_limit_bytes=60 * 2**20
        ),
    )(
        latent,
        context,
        condition.reshape(1, D),
        context_condition.reshape(1, D),
        norm_gain.reshape(1, D),
        shift_weight,
        scale_weight,
        gate_weight,
        query_weight,
        key_weight.T,
        value_weight.T,
        query_gain.reshape(1, HEAD),
        key_gain.reshape(1, HEAD),
        output_weight,
    )


def solution(mesh):
    split = Mesh(mesh.devices.reshape(NZ, NY, NX, NC), AXES)
    seq, tp, everything = ("z", "y"), ("x", "c"), AXES
    return jax.shard_map(
        on_device,
        mesh=split,
        in_specs=(
            P(everything, None),
            P(seq, None),
            P(),
            P(),
            P(),
            P(seq, tp),
            P(seq, tp),
            P(seq, tp),
            P(None, tp),
            P(None, tp),
            P(None, tp),
            P(),
            P(),
            P(),
        ),
        out_specs=P(everything, None),
        check_vma=False,
    )
```

```python
import functools
import math

import jax
import jax.numpy as jnp
from jax import lax
from jax.experimental import pallas as pl
from jax.experimental.pallas import tpu as pltpu
from jax.sharding import Mesh
from jax.sharding import PartitionSpec as P

F32 = jnp.float32
BF16 = jnp.bfloat16
MESH = pl.DeviceIdType.MESH
AXES = ("z", "y", "x", "c")
NZ, NY, NX, NC = 8, 4, 4, 2
NT = NX * NC
D = 2048
HEAD = 64
OWN = 64
TOK = OWN * NT
QUARTER = TOK // NX
ORDER = (0, -1, 1, 2)
CTX = 16
COLS = 2 * TOK
GRID_W = 64
EPS = 1e-06
LOG2E = math.log2(math.e)


def remote(src, dst, send, recv, device):
    return pltpu.make_async_remote_copy(
        src_ref=src, dst_ref=dst, send_sem=send, recv_sem=recv, device_id=device, device_id_type=MESH
    )


def column(row):
    n = row.shape[1]
    same = lax.broadcasted_iota(jnp.int32, (n, n), 0) == lax.broadcasted_iota(jnp.int32, (n, n), 1)
    return jnp.sum(jnp.where(same, jnp.broadcast_to(row, (n, n)), 0.0), axis=1, keepdims=True)


def kernel(
    latent,
    context_in,
    condition_in,
    context_condition_in,
    norm_gain_in,
    shift_w,
    scale_w,
    gate_w,
    query_w,
    key_w,
    value_w,
    query_gain_in,
    key_gain_in,
    output_w,
    out,
    context,
    condition,
    context_condition,
    norm_gain,
    query_gain,
    key_gain,
    wmod,
    wcat,
    kvw,
    wo,
    mod1,
    mod2,
    mod3,
    vecs,
    lat,
    scales,
    hid,
    tables,
    qraw,
    qhl,
    kv,
    kk,
    vt,
    ctx,
    ckk,
    cvt,
    m_ref,
    o_ref,
    s_ref,
    cs_ref,
    mx_ref,
    osend,
    lmsend,
    orecv,
    lmrecv,
    orelay,
    asend,
    arecv,
    local_sem,
    mod1_s,
    mod1_r,
    mod2_s,
    mod2_r,
    mod3_s,
    mod3_r,
    lat_s,
    lx_r,
    lf_r,
    lc_r,
    q_s,
    q_r,
    kv_s,
    kv_r,
    ctx_s,
    ctx_r,
    o_s,
    o_r,
    or_r,
    lm_s,
    lm_r,
    a_s,
    a_r,
):
    z, y, x, c = (lax.axis_index(a) for a in AXES)
    sp = z * NY + y
    tp = x * NC + c

    def at_z(d):
        return lax.rem(z + d + NZ, NZ)

    def at_y(d):
        return lax.rem(y + d + NY, NY)

    def at_x(d):
        return lax.rem(x + d + NX, NX)

    def tp_peer(d):
        t = lax.rem(tp + d, NT)
        return t, {"x": t // NC, "c": lax.rem(t, NC)}

    odd = lax.rem(sp, 2)
    half = pl.ds(pl.multiple_of(odd * 64, 64), 64)
    other_half = pl.ds(pl.multiple_of((1 - odd) * 64, 64), 64)
    loads = [
        pltpu.make_async_copy(shift_w, wmod.at[half, pl.ds(0, 256)], local_sem.at[0]),
        pltpu.make_async_copy(scale_w, wmod.at[half, pl.ds(256, 256)], local_sem.at[1]),
        pltpu.make_async_copy(gate_w, wmod.at[half, pl.ds(512, 256)], local_sem.at[2]),
        pltpu.make_async_copy(query_w, wcat.at[:, pl.ds(0, 128)], local_sem.at[3]),
        pltpu.make_async_copy(key_w, kvw.at[pl.ds(0, 64)], local_sem.at[4]),
        pltpu.make_async_copy(value_w, kvw.at[pl.ds(64, 64)], local_sem.at[5]),
        pltpu.make_async_copy(output_w, wo, local_sem.at[6]),
        pltpu.make_async_copy(latent, lat.at[tp], local_sem.at[7]),
        pltpu.make_async_copy(condition_in, condition, local_sem.at[8]),
        pltpu.make_async_copy(context_condition_in, context_condition, local_sem.at[9]),
        pltpu.make_async_copy(context_in, context, local_sem.at[10]),
        pltpu.make_async_copy(norm_gain_in, norm_gain, local_sem.at[11]),
        pltpu.make_async_copy(query_gain_in, query_gain, local_sem.at[12]),
        pltpu.make_async_copy(key_gain_in, key_gain, local_sem.at[13]),
    ]
    for i in (8, 9, 0, 1, 2, 7, 3, 4, 5, 10, 11, 12, 13, 6):
        loads[i].start()

    barrier = pltpu.get_barrier_semaphore()
    for d in range(1, NZ):
        pl.semaphore_signal(barrier, inc=1, device_id={"z": at_z(d)}, device_id_type=MESH)
    for d in range(1, NY):
        pl.semaphore_signal(barrier, inc=1, device_id={"y": at_y(d)}, device_id_type=MESH)
    for d in range(1, NT):
        pl.semaphore_signal(barrier, inc=1, device_id=tp_peer(d)[1], device_id_type=MESH)

    wmod[other_half, :] = jnp.zeros((64, 768), BF16)
    pair = pl.ds(pl.multiple_of((sp // 2) * 128, 128), 128)
    loads[8].wait()
    loads[9].wait()
    c0 = jnp.broadcast_to(condition[:, pair], (16, 128))
    c1 = jnp.broadcast_to(context_condition[:, pair], (16, 128))
    line = lax.broadcasted_iota(jnp.int32, (16, 128), 0)
    both = jnp.where(line == 0, c0, jnp.where(line == 1, c1, 0.0))
    activated = (both / (1.0 + jnp.exp(-both))).astype(BF16)
    for load in loads[:3]:
        load.wait()
    part = jnp.dot(activated, wmod[...], preferred_element_type=F32)
    rows = jnp.concatenate(
        [
            part[0:1, 0:256],
            part[0:1, 256:512],
            part[0:1, 512:768],
            part[1:2, 0:256],
            part[1:2, 256:512],
            jnp.zeros((3, 256), F32),
        ],
        axis=0,
    )
    mod1[z] = rows
    loads[7].wait()
    pl.semaphore_wait(barrier, NZ - 1 + NY - 1 + NT - 1)

    top, low = pl.ds(0, 32), pl.ds(32, 32)
    right, left = {"x": at_x(1)}, {"x": at_x(-1)}
    mate = {"c": 1 - c}

    def block_of(d):
        return at_x(d) * NC + c

    def lat_half(d, rows_):
        return lat.at[block_of(d), rows_]

    def go(copy):
        copy.start()

    go(remote(lat_half(0, top), lat_half(0, top), lat_s, lx_r.at[0], right))
    go(remote(lat_half(0, low), lat_half(0, low), lat_s, lx_r.at[1], left))
    for d in range(1, NZ):
        go(remote(mod1.at[z], mod1.at[z], mod1_s, mod1_r, {"z": at_z(d)}))
    go(remote(lat_half(0, low), lat_half(0, low), lat_s, lx_r.at[2], right))
    go(remote(lat_half(0, top), lat_half(0, top), lat_s, lx_r.at[3], left))
    go(remote(lat.at[tp], lat.at[tp], lat_s, lc_r.at[0], mate))

    loads[3].wait()
    loads[4].wait()
    loads[5].wait()
    wcat[:, 128:256] = kvw[...].T
    for load in loads[10:]:
        load.wait()
    lane = lax.broadcasted_iota(jnp.int32, (16, TOK), 1)
    freq = jnp.exp(
        lax.broadcasted_iota(jnp.int32, (16, TOK), 0).astype(F32) * (-math.log(10000.0) / 16.0)
    )
    row_angle = (lane // GRID_W + sp * (TOK // GRID_W)).astype(F32) * freq
    col_angle = lax.rem(lane, GRID_W).astype(F32) * freq
    tables[0] = jnp.cos(row_angle)
    tables[1] = jnp.sin(row_angle)
    tables[2] = jnp.cos(col_angle)
    tables[3] = jnp.sin(col_angle)
    for r in range(NZ):
        vt[r, 64:80, :] = jnp.ones((16, TOK), BF16)
    key_column, query_column = column(key_gain[...]), column(query_gain[...])
    cvt[64:80, :] = jnp.ones((16, CTX * NZ), BF16)
    m_ref[...] = jnp.full(m_ref.shape, -1e30, F32)
    o_ref[...] = jnp.zeros(o_ref.shape, F32)

    def arrived(dst, sem):
        remote(dst, dst, lat_s, sem, mate).wait_recv()

    arrived(mod1.at[pl.ds(0, NZ - 1)], mod1_r)
    mod2[y] = jnp.sum(mod1[...], axis=0)
    for d in range(1, NY):
        go(remote(mod2.at[y], mod2.at[y], mod2_s, mod2_r, {"y": at_y(d)}))

    piece = [pl.ds(16 * i, 16) for i in range(4)]

    def relay(d, i, device):
        go(remote(lat_half(d, piece[i]), lat_half(d, piece[i]), lat_s, lf_r.at[i], device))

    arrived(lat_half(-1, top), lx_r.at[0])
    relay(-1, 0, right)
    go(remote(lat_half(-1, top), lat_half(-1, top), lat_s, lc_r.at[1], mate))
    arrived(lat_half(1, low), lx_r.at[1])
    relay(1, 2, left)
    go(remote(lat_half(1, low), lat_half(1, low), lat_s, lc_r.at[2], mate))

    arrived(mod2.at[pl.ds(0, NY - 1)], mod2_r)
    mod3[tp] = jnp.sum(mod2[...], axis=0)
    for d in range(1, NT):
        t, device = tp_peer(d)
        go(remote(mod3.at[tp], mod3.at[tp], mod3_s, mod3_r, device))
    relay(-1, 1, right)
    relay(1, 3, left)

    arrived(lat_half(-1, low), lx_r.at[2])
    go(remote(lat_half(-1, low), lat_half(-1, low), lat_s, lc_r.at[3], mate))
    arrived(lat_half(1, top), lx_r.at[3])
    go(remote(lat_half(1, top), lat_half(1, top), lat_s, lc_r.at[4], mate))

    def mate_block(d):
        return at_x(d) * NC + 1 - c

    def row_scale(rows_):
        wide = rows_.astype(F32)
        return lax.rsqrt(jnp.mean(wide * wide, axis=1, keepdims=True) + EPS)

    def measure_rows(i):
        for k in range(NC):
            block = at_x(ORDER[i]) * NC + k
            scales[block] = jnp.broadcast_to(row_scale(lat[block]), (OWN, 128))

    arrived(lat.at[mate_block(0)], lc_r.at[0])
    measure_rows(0)
    arrived(lat.at[mate_block(-1), top], lc_r.at[1])
    arrived(lat.at[mate_block(-1), low], lc_r.at[3])
    measure_rows(1)
    arrived(lat.at[mate_block(1), low], lc_r.at[2])
    arrived(lat.at[mate_block(1), top], lc_r.at[4])
    measure_rows(2)
    context_scale = row_scale(context[...])

    arrived(mod3.at[pl.ds(0, NT - 1)], mod3_r)
    vec = jnp.concatenate([mod3[t] for t in range(NT)], axis=1)
    vecs[0:1] = norm_gain[...] * (1.0 + vec[1:2])
    vecs[1:2] = vec[0:1]
    vecs[2:3] = vec[2:3]
    vecs[3:4] = norm_gain[...] * (1.0 + vec[4:5])
    vecs[4:5] = vec[3:4]

    def normed(field, gain):
        mean = jnp.mean(field * field, axis=0, keepdims=True)
        return field * lax.rsqrt(mean + EPS) * gain

    up, down = {"z": at_z(1)}, {"z": at_z(-1)}
    y_of = (None, {"y": at_y(1)}, {"y": at_y(-1)}, {"y": at_y(2)})
    there = (None, 2, 1, 3)

    def part_of(i):
        return pl.ds(pl.multiple_of(at_x(ORDER[i]) * QUARTER, QUARTER), QUARTER)

    def kv_copy(slot, to, i):
        return remote(
            kv.at[slot, part_of(i)],
            kv.at[to, part_of(i)],
            kv_s,
            kv_r.at[to - 1, i],
            down if to in (2, 4, 6) or slot == 6 else up,
        )

    def kv_arrived(slot, i):
        dst = kv.at[slot, part_of(i)]
        remote(dst, dst, kv_s, kv_r.at[slot - 1, i], up).wait_recv()

    def process(quarters):
        for n, i in enumerate(quarters):
            xb = at_x(ORDER[i])
            for k in range(NC):
                block = xb * NC + k
                if i < 3:
                    scale = scales[block, :, 0:1]
                else:
                    scale = row_scale(lat[block])
                hid[QUARTER * n + OWN * k : QUARTER * n + OWN * (k + 1), :] = (
                    lat[block].astype(F32) * scale * vecs[0:1] + vecs[1:2]
                ).astype(BF16)
        many = QUARTER * len(quarters)
        if quarters[0] == 0:
            hid[many : many + CTX, :] = (
                context[...].astype(F32) * context_scale * vecs[3:4] + vecs[4:5]
            ).astype(BF16)
            many += CTX
        all_projected = jnp.dot(hid[0:many], wcat[...], preferred_element_type=F32)
        for n, i in enumerate(quarters):
            share_out(i, all_projected[QUARTER * n : QUARTER * (n + 1)].T)
        if quarters[0] == 0:
            cp = all_projected[QUARTER : QUARTER + CTX]
            ck = cp[:, 128:192]
            ck = ck * lax.rsqrt(jnp.mean(ck * ck, axis=1, keepdims=True) + EPS) * key_gain[...]
            ctx[z] = jnp.concatenate([ck, cp[:, 192:256]], axis=1).astype(BF16)
            for d in range(1, NZ):
                go(remote(ctx.at[z], ctx.at[z], ctx_s, ctx_r, {"z": at_z(d)}))

    def share_out(i, turned):
        xb = at_x(ORDER[i])
        lanes = pl.ds(pl.multiple_of(xb * QUARTER, QUARTER), QUARTER)
        cr, sr, cc, sc = (tables[k, :, lanes] for k in range(4))

        def rotated(field):
            a, b, e, f = field[0:16], field[16:32], field[32:48], field[48:64]
            return jnp.concatenate(
                [a * cr - b * sr, b * cr + a * sr, e * cc - f * sc, f * cc + e * sc], axis=0
            )

        keys = rotated(normed(turned[128:192], key_column))
        packed = jnp.concatenate([keys[:, 0:64], keys[:, 64:128]], axis=0).T
        first = pl.multiple_of(xb * QUARTER, QUARTER)
        kv[0, pl.ds(first, 64), :] = packed.astype(BF16)
        kv[0, pl.ds(first + 64, 64), :] = turned[192:256].astype(BF16)
        go(kv_copy(0, 1, i))
        go(kv_copy(0, 2, i))
        for h in range(2):
            q = rotated(normed(turned[64 * h : 64 * h + 64], query_column))
            qraw[0, xb, :, QUARTER * h : QUARTER * (h + 1)] = q.astype(BF16)
        for g in (1, 2):
            go(
                remote(
                    qraw.at[0, xb],
                    qraw.at[there[g], xb],
                    q_s,
                    q_r.at[there[g] - 1],
                    y_of[g],
                )
            )

    process((0,))

    arrived(lat_half(2, piece[0]), lf_r.at[0])
    arrived(lat_half(2, piece[1]), lf_r.at[1])
    go(remote(lat_half(2, top), lat_half(2, top), lat_s, lc_r.at[5], mate))
    arrived(lat_half(2, piece[2]), lf_r.at[2])
    arrived(lat_half(2, piece[3]), lf_r.at[3])
    go(remote(lat_half(2, low), lat_half(2, low), lat_s, lc_r.at[6], mate))

    process((1, 2))

    arrived(lat.at[mate_block(2), top], lc_r.at[5])
    arrived(lat.at[mate_block(2), low], lc_r.at[6])

    process((3,))

    def prepare_queries(g):
        for k in range(NX):
            q = qraw[g, k].astype(F32) * (LOG2E * HEAD ** (-0.5))
            high = q.astype(BF16)
            cols = slice(2 * QUARTER * k, 2 * QUARTER * (k + 1))
            qhl[g, 0:64, cols] = high
            qhl[g, 64:128, cols] = (q - high.astype(F32)).astype(BF16)

    def prepare_keys(slot):
        for k in range(NX):
            first = QUARTER * k
            packed_keys = kv[slot, first : first + 64, :]
            low_lanes, high_lanes = packed_keys[:, 0:64], packed_keys[:, 64:128]
            kk[slot, first : first + 64, :] = jnp.concatenate([low_lanes, low_lanes], axis=1)
            kk[slot, first + 64 : first + 128, :] = jnp.concatenate([high_lanes, high_lanes], axis=1)
            vt[slot, 0:64, first : first + QUARTER] = kv[slot, first + 64 : first + QUARTER, :]

    tiles = NZ * NY

    def pick(cases, default):
        for test, value in reversed(cases):
            default = jnp.where(test, value, default)
        return default

    def tile_of(t):
        w, v = t - 1 + 6, t - 19 + 20
        slot = pick(
            [(t < 1, 0), (t < 9, w // 2 - 3), (t < 13, t - 9), (t < 19, w // 3 - 2), (t < 25, 6 + lax.rem(v, 2))],
            t - 24,
        )
        group = pick(
            [(t < 1, 0), (t < 9, 1 + lax.rem(w, 2)), (t < 13, 3), (t < 19, 1 + lax.rem(w, 3)), (t < 25, 13 - v // 2)],
            0,
        )
        return slot, group

    strips = [pl.ds(256 * k, 256) for k in range(COLS // 256)]

    def score_strip(tile, side, cols):
        slot, group = tile
        s = jnp.dot(kk[slot], qhl[group, :, cols], preferred_element_type=F32)
        s_ref[side, :, cols] = s
        mx_ref[side, :, cols] = jnp.max(s, axis=0, keepdims=True)

    def absorb_strip(tile, side, cols):
        slot, group = tile
        old = m_ref[group, :, cols]
        new = jnp.maximum(old, mx_ref[side, :, cols])
        p = jnp.exp2(s_ref[side, :, cols] - new).astype(BF16)
        m_ref[group, :, cols] = new
        o_ref[group, :, cols] = o_ref[group, :, cols] * jnp.exp2(old - new) + jnp.dot(
            vt[slot], p, preferred_element_type=F32
        )

    def score(t, side):
        for cols in strips:
            score_strip(tile_of(t), side, cols)

    def absorb(t, side):
        for cols in strips:
            absorb_strip(tile_of(t), side, cols)

    def score_context(g):
        for cols in strips:
            s = jnp.dot(ckk[...], qhl[g, :, cols], preferred_element_type=F32)
            cs_ref[g, :, cols] = s + math.log2(TOK / (2.0 * CTX))

    def absorb_context(g):
        for cols in strips:
            s = cs_ref[g, :, cols]
            old = m_ref[g, :, cols]
            new = jnp.maximum(old, jnp.max(s, axis=0, keepdims=True))
            p = jnp.exp2(s - new).astype(BF16)
            m_ref[g, :, cols] = new
            o_ref[g, :, cols] = o_ref[g, :, cols] * jnp.exp2(old - new) + jnp.dot(
                cvt[...], p, preferred_element_type=F32
            )

    halves = (pl.ds(0, HEAD // 2), pl.ds(HEAD // 2, HEAD // 2))

    def relay_out():
        for k in range(2):
            remote(orelay.at[k], orelay.at[k], o_s, or_r.at[k], up).wait_recv()
            remote(orelay.at[k], orecv.at[2, halves[k]], o_s, o_r, y_of[k + 1]).start()

    def send_out(g):
        osend[g - 1] = o_ref[g, 0:64, :].astype(BF16)
        for i in range(4):
            lmsend[g - 1, i : i + 1, :] = o_ref[g, 64:65, 256 * i : 256 * (i + 1)]
            lmsend[g - 1, 4 + i : 5 + i, :] = m_ref[g, :, 256 * i : 256 * (i + 1)]
        to = there[g] - 1
        if g == 3:
            for k in range(2):
                remote(osend.at[2, halves[k]], orelay.at[k], o_s, or_r.at[k], y_of[k + 1]).start()
        else:
            remote(osend.at[g - 1], orecv.at[to], o_s, o_r, y_of[g]).start()
        remote(lmsend.at[g - 1], lmrecv.at[to], lm_s, lm_r, y_of[g]).start()

    def pass_on(i):
        for slot in (1, 2):
            kv_arrived(slot, i)
            go(kv_copy(slot, slot + 2, i))

    prepare_keys(0)
    prepare_queries(0)
    pass_on(0)
    score(0, 0)
    absorb(0, 0)

    pass_on(1)
    arrived(ctx.at[pl.ds(0, NZ - 1)], ctx_r)
    every = ctx[...].reshape(NZ * CTX, 128)
    ckk[...] = jnp.concatenate([every[:, 0:64], every[:, 0:64]], axis=1)
    cvt[0:64, :] = every.astype(F32).T[64:128].astype(BF16)
    score_context(0)
    absorb_context(0)

    pass_on(2)
    pass_on(3)
    prepare_keys(1)
    prepare_keys(2)

    def queries_arrived(g):
        remote(qraw.at[g], qraw.at[g], q_s, q_r.at[g - 1], up).wait_recv()
        prepare_queries(g)

    queries_arrived(1)
    go(remote(qraw.at[1, pl.ds(0, 2)], qraw.at[3, pl.ds(0, 2)], q_s, q_r.at[2], y_of[2]))
    score(1, 1)
    queries_arrived(2)
    go(remote(qraw.at[2, pl.ds(2, 2)], qraw.at[3, pl.ds(2, 2)], q_s, q_r.at[2], y_of[1]))

    def body(j, carry):
        @pl.when(j == 1)
        def _():
            for slot in (3, 4):
                kv_arrived(slot, 0)
                fwd(slot, 0)

        @pl.when(j == 2)
        def _():
            for i in (1, 2, 3):
                for slot in (3, 4):
                    kv_arrived(slot, i)
                    fwd(slot, i)
            prepare_keys(3)

        @pl.when(j == 3)
        def _():
            queries_arrived(3)
            prepare_keys(4)

        @pl.when(j == 5)
        def _():
            for i in (0, 1):
                kv_arrived(5, i)
                fwd(5, i)
                kv_arrived(6, i)

        @pl.when(j == 6)
        def _():
            for i in (2, 3):
                kv_arrived(6, i)
                fwd(6, i)
                kv_arrived(5, i)
            prepare_keys(5)
            prepare_keys(6)

        @pl.when(j == 9)
        def _():
            for i in range(NX):
                kv_arrived(7, i)
            prepare_keys(7)
            for g in (1, 2, 3):
                score_context(g)
            for g in (1, 2, 3):
                absorb_context(g)

        for k, g in ((10, 3), (11, 2), (12, 1)):
            pl.when(j == k)(functools.partial(send_out, g))

        pl.when(j == tiles // 2 - 3)(relay_out)

        now = tile_of(2 * j + 1)
        for u in range(2):
            t = 2 * j + 1 + u
            side = (u + 1) % 2
            following = tile_of(t + 1)
            for cols in strips:
                score_strip(following, 1 - side, cols)
                absorb_strip(now, side, cols)
            now = following
        return carry

    def fwd(slot, i):
        copy = kv_copy(slot, min(slot + 2, 7), i)
        copy.start()

    lax.fori_loop(0, tiles // 2 - 1, body, 0)
    absorb(tiles - 1, 1)

    def unpacked(i, first):
        return jnp.concatenate([lmrecv[i, first + k : first + k + 1, :] for k in range(4)], axis=1)

    top_m = m_ref[0]
    remote(lmrecv, lmrecv, lm_s, lm_r, up).wait_recv()
    for i in range(NY - 1):
        top_m = jnp.maximum(top_m, unpacked(i, 4))
    weight = jnp.exp2(m_ref[0] - top_m)
    total = o_ref[0, 64:65, :] * weight
    mixed = o_ref[0, 0:64, :] * weight
    remote(orecv, orecv, o_s, o_r, up).wait_recv()
    for i in (2, 1, 0):
        weight = jnp.exp2(unpacked(i, 4) - top_m)
        total = total + unpacked(i, 0) * weight
        mixed = mixed + orecv[i].astype(F32) * weight
    mixed = mixed / total
    for k in range(NX):
        cols = mixed[:, 2 * QUARTER * k : 2 * QUARTER * (k + 1)]
        attended = jnp.concatenate([cols[:, 0:QUARTER], cols[:, QUARTER:]], axis=0).T.astype(BF16)
        for h in range(NC):
            asend[NC * k + h] = attended[OWN * h : OWN * (h + 1)]
    arecv[tp] = asend[tp]
    for d in range(1, NT):
        t, device = tp_peer(d)
        go(remote(asend.at[t], arecv.at[tp], a_s, a_r, device))
    loads[6].wait()
    arrived(arecv.at[pl.ds(0, NT - 1)], a_r)
    heads = jnp.concatenate([arecv[t] for t in range(NT)], axis=1)
    for i in range(4):
        cols = slice(512 * i, 512 * (i + 1))
        branch = jnp.dot(heads, wo[:, cols], preferred_element_type=F32)
        out[:, cols] = (
            lat[tp, :, cols].astype(F32) + vecs[2:3, cols] * branch
        ).astype(BF16)

    for ref, sem in (
        (mod1.at[pl.ds(0, NZ - 1)], mod1_s),
        (mod2.at[pl.ds(0, NY - 1)], mod2_s),
        (mod3.at[pl.ds(0, NT - 1)], mod3_s),
        (lat.at[pl.ds(0, NT - 1)], lat_s),
        (qraw.at[pl.ds(0, NY - 1)], q_s),
        (kv.at[pl.ds(0, NZ - 1)], kv_s),
        (ctx.at[pl.ds(0, NZ - 1)], ctx_s),
        (qraw, o_s),
        (lmsend, lm_s),
        (arecv.at[pl.ds(0, NT - 1)], a_s),
    ):
        remote(ref, ref, sem, sem, up).wait_send()


def on_device(
    latent,
    context,
    condition,
    context_condition,
    norm_gain,
    shift_weight,
    scale_weight,
    gate_weight,
    query_weight,
    key_weight,
    value_weight,
    query_gain,
    key_gain,
    output_weight,
):
    hbm = pl.BlockSpec(memory_space=pl.ANY)
    dma, V = pltpu.SemaphoreType.DMA, pltpu.VMEM
    return pl.pallas_call(
        kernel,
        out_shape=pltpu.VMEM((OWN, D), BF16),
        in_specs=[hbm] * 14,
        out_specs=pl.BlockSpec(memory_space=pltpu.VMEM),
        scratch_shapes=[
            V((CTX, D), BF16),
            V((1, D), F32),
            V((1, D), F32),
            V((1, D), F32),
            V((1, HEAD), F32),
            V((1, HEAD), F32),
            V((128, 768), BF16),
            V((D, 256), BF16),
            V((128, D), BF16),
            V((1024, D), BF16),
            V((NZ, 8, 256), F32),
            V((NY, 8, 256), F32),
            V((NT, 8, 256), F32),
            V((8, D), F32),
            V((NT, OWN, D), BF16),
            V((NT, OWN, 128), F32),
            V((2 * QUARTER, D), BF16),
            V((4, 16, TOK), F32),
            V((NY, NX, HEAD, 2 * QUARTER), BF16),
            V((NY, 2 * HEAD, COLS), BF16),
            V((NZ, 512, 128), BF16),
            V((NZ, TOK, 128), BF16),
            V((NZ, 80, TOK), BF16),
            V((NZ, CTX, 128), BF16),
            V((NZ * CTX, 128), BF16),
            V((80, NZ * CTX), BF16),
            V((NY, 1, COLS), F32),
            V((NY, 80, COLS), F32),
            V((2, TOK, COLS), F32),
            V((NY, NZ * CTX, COLS), F32),
            V((2, 1, COLS), F32),
            V((NY - 1, HEAD, COLS), BF16),
            V((NY - 1, 8, 256), F32),
            V((NY - 1, HEAD, COLS), BF16),
            V((NY - 1, 8, 256), F32),
            V((2, HEAD // 2, COLS), BF16),
            V((NT, OWN, 128), BF16),
            V((NT, OWN, 128), BF16),
            dma((14,)),
            dma,
            dma,
            dma,
            dma,
            dma,
            dma,
            dma,
            dma((4,)),
            dma((4,)),
            dma((7,)),
            dma,
            dma((NY - 1,)),
            dma,
            dma((NZ - 1, NX)),
            dma,
            dma,
            dma,
            dma,
            dma((2,)),
            dma,
            dma,
            dma,
            dma,
        ],
        compiler_params=pltpu.CompilerParams(
            collective_id=0, has_side_effects=True, vmem_limit_bytes=60 * 2**20
        ),
    )(
        latent,
        context,
        condition.reshape(1, D),
        context_condition.reshape(1, D),
        norm_gain.reshape(1, D),
        shift_weight,
        scale_weight,
        gate_weight,
        query_weight,
        key_weight.T,
        value_weight.T,
        query_gain.reshape(1, HEAD),
        key_gain.reshape(1, HEAD),
        output_weight,
    )


def solution(mesh):
    split = Mesh(mesh.devices.reshape(NZ, NY, NX, NC), AXES)
    seq, tp, everything = ("z", "y"), ("x", "c"), AXES
    return jax.shard_map(
        on_device,
        mesh=split,
        in_specs=(
            P(everything, None),
            P(seq, None),
            P(),
            P(),
            P(),
            P(seq, tp),
            P(seq, tp),
            P(seq, tp),
            P(None, tp),
            P(None, tp),
            P(None, tp),
            P(),
            P(),
            P(),
        ),
        out_specs=P(everything, None),
        check_vma=False,
    )
```

```python
import functools
import math

import jax
import jax.numpy as jnp
from jax import lax
from jax.experimental import pallas as pl
from jax.experimental.pallas import tpu as pltpu
from jax.sharding import Mesh
from jax.sharding import PartitionSpec as P

F32 = jnp.float32
BF16 = jnp.bfloat16
MESH = pl.DeviceIdType.MESH
AXES = ("z", "y", "x", "c")
NZ, NY, NX, NC = 8, 4, 4, 2
NT = NX * NC
D = 2048
HEAD = 64
OWN = 64
TOK = OWN * NT
QUARTER = TOK // NX
ORDER = (0, -1, 1, 2)
CTX = 16
COLS = 2 * TOK
GRID_W = 64
EPS = 1e-06
LOG2E = math.log2(math.e)


def remote(src, dst, send, recv, device):
    return pltpu.make_async_remote_copy(
        src_ref=src, dst_ref=dst, send_sem=send, recv_sem=recv, device_id=device, device_id_type=MESH
    )


def column(row):
    n = row.shape[1]
    same = lax.broadcasted_iota(jnp.int32, (n, n), 0) == lax.broadcasted_iota(jnp.int32, (n, n), 1)
    return jnp.sum(jnp.where(same, jnp.broadcast_to(row, (n, n)), 0.0), axis=1, keepdims=True)


def kernel(
    latent,
    context_in,
    condition_in,
    context_condition_in,
    norm_gain_in,
    shift_w,
    scale_w,
    gate_w,
    query_w,
    key_w,
    value_w,
    query_gain_in,
    key_gain_in,
    output_w,
    out,
    context,
    condition,
    context_condition,
    norm_gain,
    query_gain,
    key_gain,
    wmod,
    wcat,
    kvw,
    wo,
    mod1,
    mod2,
    mod3,
    vecs,
    lat,
    scales,
    hid,
    tables,
    qraw,
    qhl,
    kv,
    kk,
    vt,
    ctx,
    m_ref,
    o_ref,
    s_ref,
    mx_ref,
    osend,
    lmsend,
    orecv,
    lmrecv,
    orelay,
    asend,
    arecv,
    local_sem,
    mod1_s,
    mod1_r,
    mod2_s,
    mod2_r,
    mod3_s,
    mod3_r,
    lat_s,
    lx_r,
    lf_r,
    lc_r,
    q_s,
    q_r,
    kv_s,
    kv_r,
    ctx_s,
    ctx_r,
    cy_s,
    cy_r,
    o_s,
    o_r,
    or_r,
    lm_s,
    lm_r,
    a_s,
    a_r,
):
    z, y, x, c = (lax.axis_index(a) for a in AXES)
    sp = z * NY + y
    tp = x * NC + c

    def at_z(d):
        return lax.rem(z + d + NZ, NZ)

    def at_y(d):
        return lax.rem(y + d + NY, NY)

    def at_x(d):
        return lax.rem(x + d + NX, NX)

    def tp_peer(d):
        t = lax.rem(tp + d, NT)
        return t, {"x": t // NC, "c": lax.rem(t, NC)}

    odd = lax.rem(sp, 2)
    half = pl.ds(pl.multiple_of(odd * 64, 64), 64)
    other_half = pl.ds(pl.multiple_of((1 - odd) * 64, 64), 64)
    loads = [
        pltpu.make_async_copy(shift_w, wmod.at[half, pl.ds(0, 256)], local_sem.at[0]),
        pltpu.make_async_copy(scale_w, wmod.at[half, pl.ds(256, 256)], local_sem.at[1]),
        pltpu.make_async_copy(gate_w, wmod.at[half, pl.ds(512, 256)], local_sem.at[2]),
        pltpu.make_async_copy(query_w, wcat.at[:, pl.ds(0, 128)], local_sem.at[3]),
        pltpu.make_async_copy(key_w, kvw.at[pl.ds(0, 64)], local_sem.at[4]),
        pltpu.make_async_copy(value_w, kvw.at[pl.ds(64, 64)], local_sem.at[5]),
        pltpu.make_async_copy(output_w, wo, local_sem.at[6]),
        pltpu.make_async_copy(latent, lat.at[tp], local_sem.at[7]),
        pltpu.make_async_copy(condition_in, condition, local_sem.at[8]),
        pltpu.make_async_copy(context_condition_in, context_condition, local_sem.at[9]),
        pltpu.make_async_copy(context_in, context, local_sem.at[10]),
        pltpu.make_async_copy(norm_gain_in, norm_gain, local_sem.at[11]),
        pltpu.make_async_copy(query_gain_in, query_gain, local_sem.at[12]),
        pltpu.make_async_copy(key_gain_in, key_gain, local_sem.at[13]),
    ]
    for i in (8, 9, 0, 1, 2, 7, 3, 4, 5, 10, 11, 12, 13, 6):
        loads[i].start()

    barrier = pltpu.get_barrier_semaphore()
    for d in range(1, NZ):
        pl.semaphore_signal(barrier, inc=1, device_id={"z": at_z(d)}, device_id_type=MESH)
    for d in range(1, NY):
        pl.semaphore_signal(barrier, inc=1, device_id={"y": at_y(d)}, device_id_type=MESH)
    for d in range(1, NT):
        pl.semaphore_signal(barrier, inc=1, device_id=tp_peer(d)[1], device_id_type=MESH)

    wmod[other_half, :] = jnp.zeros((64, 768), BF16)
    pair = pl.ds(pl.multiple_of((sp // 2) * 128, 128), 128)
    loads[8].wait()
    loads[9].wait()
    c0 = jnp.broadcast_to(condition[:, pair], (16, 128))
    c1 = jnp.broadcast_to(context_condition[:, pair], (16, 128))
    line = lax.broadcasted_iota(jnp.int32, (16, 128), 0)
    both = jnp.where(line == 0, c0, jnp.where(line == 1, c1, 0.0))
    activated = (both / (1.0 + jnp.exp(-both))).astype(BF16)
    for load in loads[:3]:
        load.wait()
    part = jnp.dot(activated, wmod[...], preferred_element_type=F32)
    rows = jnp.concatenate(
        [
            part[0:1, 0:256],
            part[0:1, 256:512],
            part[0:1, 512:768],
            part[1:2, 0:256],
            part[1:2, 256:512],
            jnp.zeros((3, 256), F32),
        ],
        axis=0,
    )
    mod1[z] = rows
    loads[7].wait()
    pl.semaphore_wait(barrier, NZ - 1 + NY - 1 + NT - 1)

    top, low = pl.ds(0, 32), pl.ds(32, 32)
    right, left = {"x": at_x(1)}, {"x": at_x(-1)}
    mate = {"c": 1 - c}

    def block_of(d):
        return at_x(d) * NC + c

    def lat_half(d, rows_):
        return lat.at[block_of(d), rows_]

    def go(copy):
        copy.start()

    go(remote(lat_half(0, top), lat_half(0, top), lat_s, lx_r.at[0], right))
    go(remote(lat_half(0, low), lat_half(0, low), lat_s, lx_r.at[1], left))
    for d in range(1, NZ):
        go(remote(mod1.at[z], mod1.at[z], mod1_s, mod1_r, {"z": at_z(d)}))
    go(remote(lat_half(0, low), lat_half(0, low), lat_s, lx_r.at[2], right))
    go(remote(lat_half(0, top), lat_half(0, top), lat_s, lx_r.at[3], left))
    go(remote(lat.at[tp], lat.at[tp], lat_s, lc_r.at[0], mate))

    loads[3].wait()
    loads[4].wait()
    loads[5].wait()
    wcat[:, 128:256] = kvw[...].T
    for load in loads[10:]:
        load.wait()
    lane = lax.broadcasted_iota(jnp.int32, (16, TOK), 1)
    freq = jnp.exp(
        lax.broadcasted_iota(jnp.int32, (16, TOK), 0).astype(F32) * (-math.log(10000.0) / 16.0)
    )
    row_angle = (lane // GRID_W + sp * (TOK // GRID_W)).astype(F32) * freq
    col_angle = lax.rem(lane, GRID_W).astype(F32) * freq
    tables[0] = jnp.cos(row_angle)
    tables[1] = jnp.sin(row_angle)
    tables[2] = jnp.cos(col_angle)
    tables[3] = jnp.sin(col_angle)
    for r in range(NZ):
        vt[r, 64:80, :] = jnp.ones((16, TOK), BF16)
    key_column, query_column = column(key_gain[...]), column(query_gain[...])
    m_ref[...] = jnp.full(m_ref.shape, -1e30, F32)
    o_ref[...] = jnp.zeros(o_ref.shape, F32)

    def arrived(dst, sem):
        remote(dst, dst, lat_s, sem, mate).wait_recv()

    arrived(mod1.at[pl.ds(0, NZ - 1)], mod1_r)
    mod2[y] = jnp.sum(mod1[...], axis=0)
    for d in range(1, NY):
        go(remote(mod2.at[y], mod2.at[y], mod2_s, mod2_r, {"y": at_y(d)}))

    piece = [pl.ds(16 * i, 16) for i in range(4)]

    def relay(d, i, device):
        go(remote(lat_half(d, piece[i]), lat_half(d, piece[i]), lat_s, lf_r.at[i], device))

    arrived(lat_half(-1, top), lx_r.at[0])
    relay(-1, 0, right)
    go(remote(lat_half(-1, top), lat_half(-1, top), lat_s, lc_r.at[1], mate))
    arrived(lat_half(1, low), lx_r.at[1])
    relay(1, 2, left)
    go(remote(lat_half(1, low), lat_half(1, low), lat_s, lc_r.at[2], mate))

    arrived(mod2.at[pl.ds(0, NY - 1)], mod2_r)
    mod3[tp] = jnp.sum(mod2[...], axis=0)
    for d in range(1, NT):
        t, device = tp_peer(d)
        go(remote(mod3.at[tp], mod3.at[tp], mod3_s, mod3_r, device))
    relay(-1, 1, right)
    relay(1, 3, left)

    arrived(lat_half(-1, low), lx_r.at[2])
    go(remote(lat_half(-1, low), lat_half(-1, low), lat_s, lc_r.at[3], mate))
    arrived(lat_half(1, top), lx_r.at[3])
    go(remote(lat_half(1, top), lat_half(1, top), lat_s, lc_r.at[4], mate))

    def mate_block(d):
        return at_x(d) * NC + 1 - c

    def row_scale(rows_):
        wide = rows_.astype(F32)
        return lax.rsqrt(jnp.mean(wide * wide, axis=1, keepdims=True) + EPS)

    def measure_rows(i):
        for k in range(NC):
            block = at_x(ORDER[i]) * NC + k
            scales[block] = jnp.broadcast_to(row_scale(lat[block]), (OWN, 128))

    arrived(lat.at[mate_block(0)], lc_r.at[0])
    measure_rows(0)
    arrived(lat.at[mate_block(-1), top], lc_r.at[1])
    arrived(lat.at[mate_block(-1), low], lc_r.at[3])
    measure_rows(1)
    arrived(lat.at[mate_block(1), low], lc_r.at[2])
    arrived(lat.at[mate_block(1), top], lc_r.at[4])
    measure_rows(2)
    context_scale = row_scale(context[...])

    arrived(mod3.at[pl.ds(0, NT - 1)], mod3_r)
    vec = jnp.concatenate([mod3[t] for t in range(NT)], axis=1)
    vecs[0:1] = norm_gain[...] * (1.0 + vec[1:2])
    vecs[1:2] = vec[0:1]
    vecs[2:3] = vec[2:3]
    vecs[3:4] = norm_gain[...] * (1.0 + vec[4:5])
    vecs[4:5] = vec[3:4]

    def normed(field, gain):
        mean = jnp.mean(field * field, axis=0, keepdims=True)
        return field * lax.rsqrt(mean + EPS) * gain

    up, down = {"z": at_z(1)}, {"z": at_z(-1)}
    y_of = (None, {"y": at_y(1)}, {"y": at_y(-1)}, {"y": at_y(2)})
    there = (None, 2, 1, 3)

    def part_of(i):
        return pl.ds(pl.multiple_of(at_x(ORDER[i]) * QUARTER, QUARTER), QUARTER)

    def kv_copy(slot, to, i):
        return remote(
            kv.at[slot, part_of(i)],
            kv.at[to, part_of(i)],
            kv_s,
            kv_r.at[to - 1, i],
            down if to in (2, 4, 6) or slot == 6 else up,
        )

    def kv_arrived(slot, i):
        dst = kv.at[slot, part_of(i)]
        remote(dst, dst, kv_s, kv_r.at[slot - 1, i], up).wait_recv()

    def process(quarters):
        for n, i in enumerate(quarters):
            xb = at_x(ORDER[i])
            for k in range(NC):
                block = xb * NC + k
                if i < 3:
                    scale = scales[block, :, 0:1]
                else:
                    scale = row_scale(lat[block])
                hid[QUARTER * n + OWN * k : QUARTER * n + OWN * (k + 1), :] = (
                    lat[block].astype(F32) * scale * vecs[0:1] + vecs[1:2]
                ).astype(BF16)
        many = QUARTER * len(quarters)
        if quarters[0] == 0:
            hid[many : many + CTX, :] = (
                context[...].astype(F32) * context_scale * vecs[3:4] + vecs[4:5]
            ).astype(BF16)
            many += CTX
        all_projected = jnp.dot(hid[0:many], wcat[...], preferred_element_type=F32)
        for n, i in enumerate(quarters):
            share_out(i, all_projected[QUARTER * n : QUARTER * (n + 1)].T)
        if quarters[0] == 0:
            cp = all_projected[QUARTER : QUARTER + CTX]
            ck = cp[:, 128:192]
            ck = ck * lax.rsqrt(jnp.mean(ck * ck, axis=1, keepdims=True) + EPS) * key_gain[...]
            ctx[y, z] = jnp.concatenate([ck, cp[:, 192:256]], axis=1).astype(BF16)
            for d in range(1, NZ):
                go(remote(ctx.at[y, z], ctx.at[y, z], ctx_s, ctx_r, {"z": at_z(d)}))

    def share_out(i, turned):
        xb = at_x(ORDER[i])
        lanes = pl.ds(pl.multiple_of(xb * QUARTER, QUARTER), QUARTER)
        cr, sr, cc, sc = (tables[k, :, lanes] for k in range(4))

        def rotated(field):
            a, b, e, f = field[0:16], field[16:32], field[32:48], field[48:64]
            return jnp.concatenate(
                [a * cr - b * sr, b * cr + a * sr, e * cc - f * sc, f * cc + e * sc], axis=0
            )

        keys = rotated(normed(turned[128:192], key_column))
        packed = jnp.concatenate([keys[:, 0:64], keys[:, 64:128]], axis=0).T
        first = pl.multiple_of(xb * QUARTER, QUARTER)
        kv[0, pl.ds(first, 64), :] = packed.astype(BF16)
        kv[0, pl.ds(first + 64, 64), :] = turned[192:256].astype(BF16)
        go(kv_copy(0, 1, i))
        go(kv_copy(0, 2, i))
        for h in range(2):
            q = rotated(normed(turned[64 * h : 64 * h + 64], query_column))
            qraw[0, xb, :, QUARTER * h : QUARTER * (h + 1)] = q.astype(BF16)
        for g in (1, 2):
            go(
                remote(
                    qraw.at[0, xb],
                    qraw.at[there[g], xb],
                    q_s,
                    q_r.at[there[g] - 1],
                    y_of[g],
                )
            )

    process((0,))

    arrived(lat_half(2, piece[0]), lf_r.at[0])
    arrived(lat_half(2, piece[1]), lf_r.at[1])
    go(remote(lat_half(2, top), lat_half(2, top), lat_s, lc_r.at[5], mate))
    arrived(lat_half(2, piece[2]), lf_r.at[2])
    arrived(lat_half(2, piece[3]), lf_r.at[3])
    go(remote(lat_half(2, low), lat_half(2, low), lat_s, lc_r.at[6], mate))

    process((1, 2))

    arrived(lat.at[mate_block(2), top], lc_r.at[5])
    arrived(lat.at[mate_block(2), low], lc_r.at[6])

    process((3,))

    def prepare_queries(g):
        for k in range(NX):
            q = qraw[g, k].astype(F32) * (LOG2E * HEAD ** (-0.5))
            high = q.astype(BF16)
            cols = slice(2 * QUARTER * k, 2 * QUARTER * (k + 1))
            qhl[g, 0:64, cols] = high
            qhl[g, 64:128, cols] = (q - high.astype(F32)).astype(BF16)

    def prepare_keys(slot):
        for k in range(NX):
            first = QUARTER * k
            packed_keys = kv[slot, first : first + 64, :]
            low_lanes, high_lanes = packed_keys[:, 0:64], packed_keys[:, 64:128]
            kk[slot, first : first + 64, :] = jnp.concatenate([low_lanes, low_lanes], axis=1)
            kk[slot, first + 64 : first + 128, :] = jnp.concatenate([high_lanes, high_lanes], axis=1)
            vt[slot, 0:64, first : first + QUARTER] = kv[slot, first + 64 : first + QUARTER, :]

    tiles = NZ * NY

    def pick(cases, default):
        for test, value in reversed(cases):
            default = jnp.where(test, value, default)
        return default

    def tile_of(t):
        w, v = t - 1 + 6, t - 19 + 20
        slot = pick(
            [(t < 1, 0), (t < 11, w // 2 - 3), (t < 16, t - 11), (t < 19, 5), (t < 25, 6 + lax.rem(v, 2))],
            t - 24,
        )
        group = pick(
            [(t < 1, 0), (t < 11, 1 + lax.rem(w, 2)), (t < 16, 3), (t < 19, t - 15), (t < 25, 13 - v // 2)],
            0,
        )
        return slot, group

    strips = [pl.ds(256 * k, 256) for k in range(COLS // 256)]

    def score_strip(tile, side, cols):
        slot, group = tile
        s = jnp.dot(kk[slot], qhl[group, :, cols], preferred_element_type=F32)
        s_ref[side, :, cols] = s
        mx_ref[side, :, cols] = jnp.max(s, axis=0, keepdims=True)

    def absorb_strip(tile, side, cols):
        slot, group = tile
        old = m_ref[group, :, cols]
        new = jnp.maximum(old, mx_ref[side, :, cols])
        p = jnp.exp2(s_ref[side, :, cols] - new).astype(BF16)
        m_ref[group, :, cols] = new
        o_ref[group, :, cols] = o_ref[group, :, cols] * jnp.exp2(old - new) + jnp.dot(
            vt[slot], p, preferred_element_type=F32
        )

    def score(t, side):
        for cols in strips:
            score_strip(tile_of(t), side, cols)

    def absorb(t, side):
        for cols in strips:
            absorb_strip(tile_of(t), side, cols)

    halves = (pl.ds(0, HEAD // 2), pl.ds(HEAD // 2, HEAD // 2))

    def relay_out():
        for k in range(2):
            remote(orelay.at[k], orelay.at[k], o_s, or_r.at[k], up).wait_recv()
            remote(orelay.at[k], orecv.at[2, halves[k]], o_s, o_r, y_of[k + 1]).start()

    def send_out(g):
        osend[g - 1] = o_ref[g, 0:64, :].astype(BF16)
        for i in range(4):
            lmsend[g - 1, i : i + 1, :] = o_ref[g, 64:65, 256 * i : 256 * (i + 1)]
            lmsend[g - 1, 4 + i : 5 + i, :] = m_ref[g, :, 256 * i : 256 * (i + 1)]
        to = there[g] - 1
        if g == 3:
            for k in range(2):
                remote(osend.at[2, halves[k]], orelay.at[k], o_s, or_r.at[k], y_of[k + 1]).start()
        else:
            remote(osend.at[g - 1], orecv.at[to], o_s, o_r, y_of[g]).start()
        remote(lmsend.at[g - 1], lmrecv.at[to], lm_s, lm_r, y_of[g]).start()

    def pass_on(i):
        for slot in (1, 2):
            kv_arrived(slot, i)
            go(kv_copy(slot, slot + 2, i))

    prepare_keys(0)
    prepare_queries(0)
    pass_on(0)
    score(0, 0)
    absorb(0, 0)

    pass_on(1)
    arrived(ctx.at[0, pl.ds(0, NZ - 1)], ctx_r)
    for g in range(1, NY):
        go(remote(ctx.at[y], ctx.at[y], cy_s, cy_r, y_of[g]))

    pass_on(2)
    pass_on(3)
    prepare_keys(1)
    prepare_keys(2)

    def queries_arrived(g):
        remote(qraw.at[g], qraw.at[g], q_s, q_r.at[g - 1], up).wait_recv()
        prepare_queries(g)

    queries_arrived(1)
    go(remote(qraw.at[1, pl.ds(0, 2)], qraw.at[3, pl.ds(0, 2)], q_s, q_r.at[2], y_of[2]))
    score(1, 1)
    queries_arrived(2)
    go(remote(qraw.at[2, pl.ds(2, 2)], qraw.at[3, pl.ds(2, 2)], q_s, q_r.at[2], y_of[1]))

    def fwd(slot, i):
        copy = kv_copy(slot, min(slot + 2, 7), i)
        copy.start()

    def take(*chunks):
        for slot, i, forward in chunks:
            kv_arrived(slot, i)
            if forward:
                fwd(slot, i)

    def far_keys_0():
        take((3, 0, True), (4, 0, True), (3, 1, True), (4, 1, True))

    def far_keys_1():
        take((3, 2, True), (4, 2, True), (3, 3, True), (4, 3, True))
        prepare_keys(3)
        prepare_keys(4)

    def far_keys_2():
        queries_arrived(3)
        take((5, 0, True), (5, 1, True), (6, 0, False), (6, 1, False), (6, 2, True), (6, 3, True))

    def far_keys_3():
        take((5, 2, False), (5, 3, False))
        prepare_keys(5)
        prepare_keys(6)

    def context_keys():
        arrived(ctx.at[pl.ds(0, NY - 1)], cy_r)
        every = ctx[...].reshape(TOK, 128)
        kk[NZ] = jnp.concatenate([every[:, 0:64], every[:, 0:64]], axis=1)
        weight = TOK / (2.0 * CTX)
        vt[NZ, 0:64, :] = (every.astype(F32).T[64:128] * weight).astype(BF16)
        vt[NZ, 64:80, :] = jnp.full((16, TOK), weight, BF16)

    def farthest_keys():
        take((7, 0, False), (7, 1, False), (7, 2, False), (7, 3, False))
        prepare_keys(7)

    def tiles_from(start, stop, each, events):
        def body(j, carry):
            for k, event in events:
                pl.when(j == k)(event)
            now = tile_of(start + each * j)
            for u in range(each):
                side = (start + u) % 2
                following = tile_of(start + each * j + u + 1)
                for cols in strips:
                    score_strip(following, 1 - side, cols)
                    absorb_strip(now, side, cols)
                now = following
            return carry

        lax.fori_loop(0, (stop - start) // each, body, 0)

    tiles_from(
        1, 21, 4, ((0, far_keys_0), (1, far_keys_1), (2, far_keys_2), (3, far_keys_3), (4, farthest_keys))
    )

    tiles_from(
        21,
        31,
        2,
        (
            (0, functools.partial(send_out, 3)),
            (1, functools.partial(send_out, 2)),
            (2, functools.partial(send_out, 1)),
            (3, relay_out),
            (4, context_keys),
        ),
    )

    for cols in strips:
        score_strip(tile_of(tiles), 0, cols)
        absorb_strip(tile_of(tiles - 1), 1, cols)
    absorb(tiles, 0)

    def unpacked(i, first):
        return jnp.concatenate([lmrecv[i, first + k : first + k + 1, :] for k in range(4)], axis=1)

    top_m = m_ref[0]
    remote(lmrecv, lmrecv, lm_s, lm_r, up).wait_recv()
    for i in range(NY - 1):
        top_m = jnp.maximum(top_m, unpacked(i, 4))
    weight = jnp.exp2(m_ref[0] - top_m)
    total = o_ref[0, 64:65, :] * weight
    mixed = o_ref[0, 0:64, :] * weight
    remote(orecv, orecv, o_s, o_r, up).wait_recv()
    for i in (2, 1, 0):
        weight = jnp.exp2(unpacked(i, 4) - top_m)
        total = total + unpacked(i, 0) * weight
        mixed = mixed + orecv[i].astype(F32) * weight
    mixed = mixed / total
    for k in range(NX):
        cols = mixed[:, 2 * QUARTER * k : 2 * QUARTER * (k + 1)]
        attended = jnp.concatenate([cols[:, 0:QUARTER], cols[:, QUARTER:]], axis=0).T.astype(BF16)
        for h in range(NC):
            asend[NC * k + h] = attended[OWN * h : OWN * (h + 1)]
    arecv[tp] = asend[tp]
    for d in range(1, NT):
        t, device = tp_peer(d)
        go(remote(asend.at[t], arecv.at[tp], a_s, a_r, device))
    loads[6].wait()
    arrived(arecv.at[pl.ds(0, NT - 1)], a_r)
    heads = jnp.concatenate([arecv[t] for t in range(NT)], axis=1)
    for i in range(4):
        cols = slice(512 * i, 512 * (i + 1))
        branch = jnp.dot(heads, wo[:, cols], preferred_element_type=F32)
        out[:, cols] = (
            lat[tp, :, cols].astype(F32) + vecs[2:3, cols] * branch
        ).astype(BF16)

    for ref, sem in (
        (mod1.at[pl.ds(0, NZ - 1)], mod1_s),
        (mod2.at[pl.ds(0, NY - 1)], mod2_s),
        (mod3.at[pl.ds(0, NT - 1)], mod3_s),
        (lat.at[pl.ds(0, NT - 1)], lat_s),
        (qraw.at[pl.ds(0, NY - 1)], q_s),
        (kv.at[pl.ds(0, NZ - 1)], kv_s),
        (ctx.at[0, pl.ds(0, NZ - 1)], ctx_s),
        (ctx.at[pl.ds(0, NY - 1)], cy_s),
        (qraw, o_s),
        (lmsend, lm_s),
        (arecv.at[pl.ds(0, NT - 1)], a_s),
    ):
        remote(ref, ref, sem, sem, up).wait_send()


def on_device(
    latent,
    context,
    condition,
    context_condition,
    norm_gain,
    shift_weight,
    scale_weight,
    gate_weight,
    query_weight,
    key_weight,
    value_weight,
    query_gain,
    key_gain,
    output_weight,
):
    hbm = pl.BlockSpec(memory_space=pl.ANY)
    dma, V = pltpu.SemaphoreType.DMA, pltpu.VMEM
    return pl.pallas_call(
        kernel,
        out_shape=pltpu.VMEM((OWN, D), BF16),
        in_specs=[hbm] * 14,
        out_specs=pl.BlockSpec(memory_space=pltpu.VMEM),
        scratch_shapes=[
            V((CTX, D), BF16),
            V((1, D), F32),
            V((1, D), F32),
            V((1, D), F32),
            V((1, HEAD), F32),
            V((1, HEAD), F32),
            V((128, 768), BF16),
            V((D, 256), BF16),
            V((128, D), BF16),
            V((1024, D), BF16),
            V((NZ, 8, 256), F32),
            V((NY, 8, 256), F32),
            V((NT, 8, 256), F32),
            V((8, D), F32),
            V((NT, OWN, D), BF16),
            V((NT, OWN, 128), F32),
            V((2 * QUARTER, D), BF16),
            V((4, 16, TOK), F32),
            V((NY, NX, HEAD, 2 * QUARTER), BF16),
            V((NY, 2 * HEAD, COLS), BF16),
            V((NZ, 512, 128), BF16),
            V((NZ + 1, TOK, 128), BF16),
            V((NZ + 1, 80, TOK), BF16),
            V((NY, NZ, CTX, 128), BF16),
            V((NY, 1, COLS), F32),
            V((NY, 80, COLS), F32),
            V((2, TOK, COLS), F32),
            V((2, 1, COLS), F32),
            V((NY - 1, HEAD, COLS), BF16),
            V((NY - 1, 8, 256), F32),
            V((NY - 1, HEAD, COLS), BF16),
            V((NY - 1, 8, 256), F32),
            V((2, HEAD // 2, COLS), BF16),
            V((NT, OWN, 128), BF16),
            V((NT, OWN, 128), BF16),
            dma((14,)),
            dma,
            dma,
            dma,
            dma,
            dma,
            dma,
            dma,
            dma((4,)),
            dma((4,)),
            dma((7,)),
            dma,
            dma((NY - 1,)),
            dma,
            dma((NZ - 1, NX)),
            dma,
            dma,
            dma,
            dma,
            dma,
            dma,
            dma((2,)),
            dma,
            dma,
            dma,
            dma,
        ],
        compiler_params=pltpu.CompilerParams(
            collective_id=0, has_side_effects=True, vmem_limit_bytes=60 * 2**20
        ),
    )(
        latent,
        context,
        condition.reshape(1, D),
        context_condition.reshape(1, D),
        norm_gain.reshape(1, D),
        shift_weight,
        scale_weight,
        gate_weight,
        query_weight,
        key_weight.T,
        value_weight.T,
        query_gain.reshape(1, HEAD),
        key_gain.reshape(1, HEAD),
        output_weight,
    )


def solution(mesh):
    split = Mesh(mesh.devices.reshape(NZ, NY, NX, NC), AXES)
    seq, tp, everything = ("z", "y"), ("x", "c"), AXES
    return jax.shard_map(
        on_device,
        mesh=split,
        in_specs=(
            P(everything, None),
            P(seq, None),
            P(),
            P(),
            P(),
            P(seq, tp),
            P(seq, tp),
            P(seq, tp),
            P(None, tp),
            P(None, tp),
            P(None, tp),
            P(),
            P(),
            P(),
        ),
        out_specs=P(everything, None),
        check_vma=False,
    )
```

```python
import functools
import math

import jax
import jax.numpy as jnp
from jax import lax
from jax.experimental import pallas as pl
from jax.experimental.pallas import tpu as pltpu
from jax.sharding import Mesh
from jax.sharding import PartitionSpec as P

F32 = jnp.float32
BF16 = jnp.bfloat16
MESH = pl.DeviceIdType.MESH
AXES = ("z", "y", "x", "c")
NZ, NY, NX, NC = 8, 4, 4, 2
NT = NX * NC
D = 2048
HEAD = 64
OWN = 64
TOK = OWN * NT
QUARTER = TOK // NX
ORDER = (0, -1, 1, 2)
CTX = 16
COLS = 2 * TOK
GRID_W = 64
EPS = 1e-06
LOG2E = math.log2(math.e)


def remote(src, dst, send, recv, device):
    return pltpu.make_async_remote_copy(
        src_ref=src, dst_ref=dst, send_sem=send, recv_sem=recv, device_id=device, device_id_type=MESH
    )


def column(row):
    n = row.shape[1]
    same = lax.broadcasted_iota(jnp.int32, (n, n), 0) == lax.broadcasted_iota(jnp.int32, (n, n), 1)
    return jnp.sum(jnp.where(same, jnp.broadcast_to(row, (n, n)), 0.0), axis=1, keepdims=True)


def kernel(
    latent,
    context_in,
    condition_in,
    context_condition_in,
    norm_gain_in,
    shift_w,
    scale_w,
    gate_w,
    query_w,
    key_w,
    value_w,
    query_gain_in,
    key_gain_in,
    output_w,
    out,
    context,
    condition,
    context_condition,
    norm_gain,
    query_gain,
    key_gain,
    wmod,
    wcat,
    kvw,
    wo,
    mod1,
    mod2,
    mod3,
    vecs,
    lat,
    scales,
    hid,
    tables,
    qraw,
    qhl,
    kv,
    kk,
    vt,
    ctx,
    m_ref,
    o_ref,
    s_ref,
    mx_ref,
    osend,
    lmsend,
    orecv,
    lmrecv,
    orelay,
    asend,
    arecv,
    local_sem,
    mod1_s,
    mod1_r,
    mod2_s,
    mod2_r,
    mod3_s,
    mod3_r,
    lat_s,
    lx_r,
    lf_r,
    lc_r,
    q_s,
    q_r,
    kv_s,
    kv_r,
    ctx_s,
    ctx_r,
    cy_s,
    cy_r,
    o_s,
    o_r,
    or_r,
    lm_s,
    lm_r,
    a_s,
    a_r,
):
    z, y, x, c = (lax.axis_index(a) for a in AXES)
    sp = z * NY + y
    tp = x * NC + c

    def at_z(d):
        return lax.rem(z + d + NZ, NZ)

    def at_y(d):
        return lax.rem(y + d + NY, NY)

    def at_x(d):
        return lax.rem(x + d + NX, NX)

    def tp_peer(d):
        t = lax.rem(tp + d, NT)
        return t, {"x": t // NC, "c": lax.rem(t, NC)}

    odd = lax.rem(sp, 2)
    half = pl.ds(pl.multiple_of(odd * 64, 64), 64)
    other_half = pl.ds(pl.multiple_of((1 - odd) * 64, 64), 64)
    loads = [
        pltpu.make_async_copy(shift_w, wmod.at[half, pl.ds(0, 256)], local_sem.at[0]),
        pltpu.make_async_copy(scale_w, wmod.at[half, pl.ds(256, 256)], local_sem.at[1]),
        pltpu.make_async_copy(gate_w, wmod.at[half, pl.ds(512, 256)], local_sem.at[2]),
        pltpu.make_async_copy(query_w, wcat.at[:, pl.ds(0, 128)], local_sem.at[3]),
        pltpu.make_async_copy(key_w, kvw.at[pl.ds(0, 64)], local_sem.at[4]),
        pltpu.make_async_copy(value_w, kvw.at[pl.ds(64, 64)], local_sem.at[5]),
        pltpu.make_async_copy(output_w, wo, local_sem.at[6]),
        pltpu.make_async_copy(latent, lat.at[tp], local_sem.at[7]),
        pltpu.make_async_copy(condition_in, condition, local_sem.at[8]),
        pltpu.make_async_copy(context_condition_in, context_condition, local_sem.at[9]),
        pltpu.make_async_copy(context_in, context, local_sem.at[10]),
        pltpu.make_async_copy(norm_gain_in, norm_gain, local_sem.at[11]),
        pltpu.make_async_copy(query_gain_in, query_gain, local_sem.at[12]),
        pltpu.make_async_copy(key_gain_in, key_gain, local_sem.at[13]),
    ]
    for i in (8, 9, 0, 1, 2, 7, 3, 4, 5, 10, 11, 12, 13, 6):
        loads[i].start()

    barrier = pltpu.get_barrier_semaphore()
    for d in range(1, NZ):
        pl.semaphore_signal(barrier, inc=1, device_id={"z": at_z(d)}, device_id_type=MESH)
    for d in range(1, NY):
        pl.semaphore_signal(barrier, inc=1, device_id={"y": at_y(d)}, device_id_type=MESH)
    for d in range(1, NT):
        pl.semaphore_signal(barrier, inc=1, device_id=tp_peer(d)[1], device_id_type=MESH)

    wmod[other_half, :] = jnp.zeros((64, 768), BF16)
    pair = pl.ds(pl.multiple_of((sp // 2) * 128, 128), 128)
    loads[8].wait()
    loads[9].wait()
    c0 = jnp.broadcast_to(condition[:, pair], (16, 128))
    c1 = jnp.broadcast_to(context_condition[:, pair], (16, 128))
    line = lax.broadcasted_iota(jnp.int32, (16, 128), 0)
    both = jnp.where(line == 0, c0, jnp.where(line == 1, c1, 0.0))
    activated = (both / (1.0 + jnp.exp(-both))).astype(BF16)
    for load in loads[:3]:
        load.wait()
    part = jnp.dot(activated, wmod[...], preferred_element_type=F32)
    rows = jnp.concatenate(
        [
            part[0:1, 0:256],
            part[0:1, 256:512],
            part[0:1, 512:768],
            part[1:2, 0:256],
            part[1:2, 256:512],
            jnp.zeros((3, 256), F32),
        ],
        axis=0,
    )
    mod1[z] = rows
    loads[7].wait()
    pl.semaphore_wait(barrier, NZ - 1 + NY - 1 + NT - 1)

    top, low = pl.ds(0, 32), pl.ds(32, 32)
    right, left = {"x": at_x(1)}, {"x": at_x(-1)}
    mate = {"c": 1 - c}

    def block_of(d):
        return at_x(d) * NC + c

    def lat_half(d, rows_):
        return lat.at[block_of(d), rows_]

    def go(copy):
        copy.start()

    go(remote(lat_half(0, top), lat_half(0, top), lat_s, lx_r.at[0], right))
    go(remote(lat_half(0, low), lat_half(0, low), lat_s, lx_r.at[1], left))
    for d in range(1, NZ):
        go(remote(mod1.at[z], mod1.at[z], mod1_s, mod1_r, {"z": at_z(d)}))
    go(remote(lat_half(0, low), lat_half(0, low), lat_s, lx_r.at[2], right))
    go(remote(lat_half(0, top), lat_half(0, top), lat_s, lx_r.at[3], left))
    go(remote(lat.at[tp], lat.at[tp], lat_s, lc_r.at[0], mate))

    loads[3].wait()
    loads[4].wait()
    loads[5].wait()
    wcat[:, 128:256] = kvw[...].T
    for load in loads[10:]:
        load.wait()
    lane = lax.broadcasted_iota(jnp.int32, (16, TOK), 1)
    freq = jnp.exp(
        lax.broadcasted_iota(jnp.int32, (16, TOK), 0).astype(F32) * (-math.log(10000.0) / 16.0)
    )
    row_angle = (lane // GRID_W + sp * (TOK // GRID_W)).astype(F32) * freq
    col_angle = lax.rem(lane, GRID_W).astype(F32) * freq
    tables[0] = jnp.cos(row_angle)
    tables[1] = jnp.sin(row_angle)
    tables[2] = jnp.cos(col_angle)
    tables[3] = jnp.sin(col_angle)
    for r in range(NZ):
        vt[r, 64:80, :] = jnp.ones((16, TOK), BF16)
    key_column, query_column = column(key_gain[...]), column(query_gain[...])
    m_ref[...] = jnp.full(m_ref.shape, -1e30, F32)
    o_ref[...] = jnp.zeros(o_ref.shape, F32)

    def arrived(dst, sem):
        remote(dst, dst, lat_s, sem, mate).wait_recv()

    arrived(mod1.at[pl.ds(0, NZ - 1)], mod1_r)
    mod2[y] = jnp.sum(mod1[...], axis=0)
    for d in range(1, NY):
        go(remote(mod2.at[y], mod2.at[y], mod2_s, mod2_r, {"y": at_y(d)}))

    piece = [pl.ds(16 * i, 16) for i in range(4)]

    def relay(d, i, device):
        go(remote(lat_half(d, piece[i]), lat_half(d, piece[i]), lat_s, lf_r.at[i], device))

    arrived(lat_half(-1, top), lx_r.at[0])
    relay(-1, 0, right)
    go(remote(lat_half(-1, top), lat_half(-1, top), lat_s, lc_r.at[1], mate))
    arrived(lat_half(1, low), lx_r.at[1])
    relay(1, 2, left)
    go(remote(lat_half(1, low), lat_half(1, low), lat_s, lc_r.at[2], mate))

    arrived(mod2.at[pl.ds(0, NY - 1)], mod2_r)
    mod3[tp] = jnp.sum(mod2[...], axis=0)
    for d in range(1, NT):
        t, device = tp_peer(d)
        go(remote(mod3.at[tp], mod3.at[tp], mod3_s, mod3_r, device))
    relay(-1, 1, right)
    relay(1, 3, left)

    arrived(lat_half(-1, low), lx_r.at[2])
    go(remote(lat_half(-1, low), lat_half(-1, low), lat_s, lc_r.at[3], mate))
    arrived(lat_half(1, top), lx_r.at[3])
    go(remote(lat_half(1, top), lat_half(1, top), lat_s, lc_r.at[4], mate))

    def mate_block(d):
        return at_x(d) * NC + 1 - c

    def row_scale(rows_):
        wide = rows_.astype(F32)
        return lax.rsqrt(jnp.mean(wide * wide, axis=1, keepdims=True) + EPS)

    def measure_rows(i):
        for k in range(NC):
            block = at_x(ORDER[i]) * NC + k
            scales[block] = jnp.broadcast_to(row_scale(lat[block]), (OWN, 128))

    arrived(lat.at[mate_block(0)], lc_r.at[0])
    measure_rows(0)
    arrived(lat.at[mate_block(-1), top], lc_r.at[1])
    arrived(lat.at[mate_block(-1), low], lc_r.at[3])
    measure_rows(1)
    arrived(lat.at[mate_block(1), low], lc_r.at[2])
    arrived(lat.at[mate_block(1), top], lc_r.at[4])
    measure_rows(2)
    context_scale = row_scale(context[...])

    arrived(mod3.at[pl.ds(0, NT - 1)], mod3_r)
    vec = jnp.concatenate([mod3[t] for t in range(NT)], axis=1)
    vecs[0:1] = norm_gain[...] * (1.0 + vec[1:2])
    vecs[1:2] = vec[0:1]
    vecs[2:3] = vec[2:3]
    vecs[3:4] = norm_gain[...] * (1.0 + vec[4:5])
    vecs[4:5] = vec[3:4]

    def normed(field, gain):
        mean = jnp.mean(field * field, axis=0, keepdims=True)
        return field * lax.rsqrt(mean + EPS) * gain

    up, down = {"z": at_z(1)}, {"z": at_z(-1)}
    y_of = (None, {"y": at_y(1)}, {"y": at_y(-1)}, {"y": at_y(2)})
    there = (None, 2, 1, 3)

    def part_of(i):
        return pl.ds(pl.multiple_of(at_x(ORDER[i]) * QUARTER, QUARTER), QUARTER)

    def kv_copy(slot, to, i):
        return remote(
            kv.at[slot, part_of(i)],
            kv.at[to, part_of(i)],
            kv_s,
            kv_r.at[to - 1, i],
            down if to in (2, 4, 6) or slot == 6 else up,
        )

    def kv_arrived(slot, i):
        dst = kv.at[slot, part_of(i)]
        remote(dst, dst, kv_s, kv_r.at[slot - 1, i], up).wait_recv()

    def process(quarters):
        for n, i in enumerate(quarters):
            xb = at_x(ORDER[i])
            for k in range(NC):
                block = xb * NC + k
                if i < 3:
                    scale = scales[block, :, 0:1]
                else:
                    scale = row_scale(lat[block])
                hid[QUARTER * n + OWN * k : QUARTER * n + OWN * (k + 1), :] = (
                    lat[block].astype(F32) * scale * vecs[0:1] + vecs[1:2]
                ).astype(BF16)
        many = QUARTER * len(quarters)
        if quarters[0] == 0:
            hid[many : many + CTX, :] = (
                context[...].astype(F32) * context_scale * vecs[3:4] + vecs[4:5]
            ).astype(BF16)
            many += CTX
        all_projected = jnp.dot(hid[0:many], wcat[...], preferred_element_type=F32)
        for n, i in enumerate(quarters):
            share_out(i, all_projected[QUARTER * n : QUARTER * (n + 1)].T)
        if quarters[0] == 0:
            cp = all_projected[QUARTER : QUARTER + CTX]
            ck = cp[:, 128:192]
            ck = ck * lax.rsqrt(jnp.mean(ck * ck, axis=1, keepdims=True) + EPS) * key_gain[...]
            ctx[y, z] = jnp.concatenate([ck, cp[:, 192:256]], axis=1).astype(BF16)
            for d in range(1, NZ):
                go(remote(ctx.at[y, z], ctx.at[y, z], ctx_s, ctx_r, {"z": at_z(d)}))

    def share_out(i, turned):
        xb = at_x(ORDER[i])
        lanes = pl.ds(pl.multiple_of(xb * QUARTER, QUARTER), QUARTER)
        cr, sr, cc, sc = (tables[k, :, lanes] for k in range(4))

        def rotated(field):
            a, b, e, f = field[0:16], field[16:32], field[32:48], field[48:64]
            return jnp.concatenate(
                [a * cr - b * sr, b * cr + a * sr, e * cc - f * sc, f * cc + e * sc], axis=0
            )

        keys = rotated(normed(turned[128:192], key_column))
        packed = jnp.concatenate([keys[:, 0:64], keys[:, 64:128]], axis=0).T
        first = pl.multiple_of(xb * QUARTER, QUARTER)
        kv[0, pl.ds(first, 64), :] = packed.astype(BF16)
        kv[0, pl.ds(first + 64, 64), :] = turned[192:256].astype(BF16)
        go(kv_copy(0, 1, i))
        go(kv_copy(0, 2, i))
        for h in range(2):
            q = rotated(normed(turned[64 * h : 64 * h + 64], query_column))
            qraw[0, xb, :, QUARTER * h : QUARTER * (h + 1)] = q.astype(BF16)
        for g in (1, 2):
            go(
                remote(
                    qraw.at[0, xb],
                    qraw.at[there[g], xb],
                    q_s,
                    q_r.at[there[g] - 1],
                    y_of[g],
                )
            )

    process((0,))

    arrived(lat_half(2, piece[0]), lf_r.at[0])
    arrived(lat_half(2, piece[1]), lf_r.at[1])
    go(remote(lat_half(2, top), lat_half(2, top), lat_s, lc_r.at[5], mate))
    arrived(lat_half(2, piece[2]), lf_r.at[2])
    arrived(lat_half(2, piece[3]), lf_r.at[3])
    go(remote(lat_half(2, low), lat_half(2, low), lat_s, lc_r.at[6], mate))

    process((1, 2))

    arrived(lat.at[mate_block(2), top], lc_r.at[5])
    arrived(lat.at[mate_block(2), low], lc_r.at[6])

    process((3,))

    def prepare_queries(g):
        for k in range(NX):
            q = qraw[g, k].astype(F32) * (LOG2E * HEAD ** (-0.5))
            high = q.astype(BF16)
            cols = slice(2 * QUARTER * k, 2 * QUARTER * (k + 1))
            qhl[g, 0:64, cols] = high
            qhl[g, 64:128, cols] = (q - high.astype(F32)).astype(BF16)

    def prepare_keys(slot):
        for k in range(NX):
            first = QUARTER * k
            packed_keys = kv[slot, first : first + 64, :]
            low_lanes, high_lanes = packed_keys[:, 0:64], packed_keys[:, 64:128]
            kk[slot, first : first + 64, :] = jnp.concatenate([low_lanes, low_lanes], axis=1)
            kk[slot, first + 64 : first + 128, :] = jnp.concatenate([high_lanes, high_lanes], axis=1)
            vt[slot, 0:64, first : first + QUARTER] = kv[slot, first + 64 : first + QUARTER, :]

    tiles = NZ * NY

    def pick(cases, default):
        for test, value in reversed(cases):
            default = jnp.where(test, value, default)
        return default

    def tile_of(t):
        w, v = t - 1 + 6, t - 19 + 20
        slot = pick(
            [(t < 1, 0), (t < 11, w // 2 - 3), (t < 16, t - 11), (t < 19, 5), (t < 25, 6 + lax.rem(v, 2))],
            t - 24,
        )
        group = pick(
            [(t < 1, 0), (t < 11, 1 + lax.rem(w, 2)), (t < 16, 3), (t < 19, t - 15), (t < 25, 13 - v // 2)],
            0,
        )
        return slot, group

    strips = [pl.ds(256 * k, 256) for k in range(COLS // 256)]

    def score_strip(tile, side, cols):
        slot, group = tile
        s = jnp.dot(kk[slot], qhl[group, :, cols], preferred_element_type=F32)
        s_ref[side, :, cols] = s
        mx_ref[side, :, cols] = jnp.max(s, axis=0, keepdims=True)

    def absorb_strip(tile, side, cols):
        slot, group = tile
        old = m_ref[group, :, cols]
        new = jnp.maximum(old, mx_ref[side, :, cols])
        p = jnp.exp2(s_ref[side, :, cols] - new).astype(BF16)
        m_ref[group, :, cols] = new
        o_ref[group, :, cols] = o_ref[group, :, cols] * jnp.exp2(old - new) + jnp.dot(
            vt[slot], p, preferred_element_type=F32
        )

    def score(t, side):
        for cols in strips:
            score_strip(tile_of(t), side, cols)

    def absorb(t, side):
        for cols in strips:
            absorb_strip(tile_of(t), side, cols)

    halves = (pl.ds(0, HEAD // 2), pl.ds(HEAD // 2, HEAD // 2))

    def relay_out():
        for k in range(2):
            remote(orelay.at[k], orelay.at[k], o_s, or_r.at[k], up).wait_recv()
            remote(orelay.at[k], orecv.at[2, halves[k]], o_s, o_r, y_of[k + 1]).start()

    def send_out(g):
        osend[g - 1] = o_ref[g, 0:64, :].astype(BF16)
        for i in range(4):
            lmsend[g - 1, i : i + 1, :] = o_ref[g, 64:65, 256 * i : 256 * (i + 1)]
            lmsend[g - 1, 4 + i : 5 + i, :] = m_ref[g, :, 256 * i : 256 * (i + 1)]
        to = there[g] - 1
        if g == 3:
            for k in range(2):
                remote(osend.at[2, halves[k]], orelay.at[k], o_s, or_r.at[k], y_of[k + 1]).start()
        else:
            remote(osend.at[g - 1], orecv.at[to], o_s, o_r, y_of[g]).start()
        remote(lmsend.at[g - 1], lmrecv.at[to], lm_s, lm_r, y_of[g]).start()

    def pass_on(i):
        for slot in (1, 2):
            kv_arrived(slot, i)
            go(kv_copy(slot, slot + 2, i))

    prepare_keys(0)
    prepare_queries(0)
    pass_on(0)
    score(0, 0)
    absorb(0, 0)

    pass_on(1)
    arrived(ctx.at[0, pl.ds(0, NZ - 1)], ctx_r)
    for g in range(1, NY):
        go(remote(ctx.at[y], ctx.at[y], cy_s, cy_r, y_of[g]))

    pass_on(2)
    pass_on(3)
    prepare_keys(1)
    prepare_keys(2)

    def queries_arrived(g):
        remote(qraw.at[g], qraw.at[g], q_s, q_r.at[g - 1], up).wait_recv()
        prepare_queries(g)

    queries_arrived(1)
    go(remote(qraw.at[1, pl.ds(0, 2)], qraw.at[3, pl.ds(0, 2)], q_s, q_r.at[2], y_of[2]))
    score(1, 1)
    queries_arrived(2)
    go(remote(qraw.at[2, pl.ds(2, 2)], qraw.at[3, pl.ds(2, 2)], q_s, q_r.at[2], y_of[1]))

    def fwd(slot, i):
        copy = kv_copy(slot, min(slot + 2, 7), i)
        copy.start()

    def take(*chunks):
        for slot, i, forward in chunks:
            kv_arrived(slot, i)
            if forward:
                fwd(slot, i)

    def far_keys_0():
        take((3, 0, True), (4, 0, True))

    def far_keys_1():
        for i in (1, 2, 3):
            take((3, i, True), (4, i, True))
        prepare_keys(3)
        prepare_keys(4)

    def far_keys_2():
        queries_arrived(3)
        take((5, 0, True), (5, 1, True), (6, 0, False), (6, 1, False), (6, 2, True), (6, 3, True))

    def far_keys_3():
        take((5, 2, False), (5, 3, False))
        prepare_keys(5)
        prepare_keys(6)

    def context_keys():
        arrived(ctx.at[pl.ds(0, NY - 1)], cy_r)
        every = ctx[...].reshape(TOK, 128)
        kk[NZ] = jnp.concatenate([every[:, 0:64], every[:, 0:64]], axis=1)
        weight = TOK / (2.0 * CTX)
        vt[NZ, 0:64, :] = (every.astype(F32).T[64:128] * weight).astype(BF16)
        vt[NZ, 64:80, :] = jnp.full((16, TOK), weight, BF16)

    def farthest_keys():
        take((7, 0, False), (7, 1, False), (7, 2, False), (7, 3, False))
        prepare_keys(7)

    def tiles_from(start, stop, each, events):
        def body(j, carry):
            for k, event in events:
                pl.when(j == k)(event)
            now = tile_of(start + each * j)
            for u in range(each):
                side = (start + u) % 2
                following = tile_of(start + each * j + u + 1)
                for cols in strips:
                    score_strip(following, 1 - side, cols)
                    absorb_strip(now, side, cols)
                now = following
            return carry

        lax.fori_loop(0, (stop - start) // each, body, 0)

    tiles_from(
        1, 21, 4, ((0, far_keys_0), (1, far_keys_1), (2, far_keys_2), (3, far_keys_3), (4, farthest_keys))
    )

    tiles_from(
        21,
        31,
        2,
        (
            (0, functools.partial(send_out, 3)),
            (1, functools.partial(send_out, 2)),
            (2, functools.partial(send_out, 1)),
            (3, relay_out),
            (4, context_keys),
        ),
    )

    for cols in strips:
        score_strip(tile_of(tiles), 0, cols)
        absorb_strip(tile_of(tiles - 1), 1, cols)
    absorb(tiles, 0)

    def unpacked(i, first):
        return jnp.concatenate([lmrecv[i, first + k : first + k + 1, :] for k in range(4)], axis=1)

    top_m = m_ref[0]
    remote(lmrecv, lmrecv, lm_s, lm_r, up).wait_recv()
    for i in range(NY - 1):
        top_m = jnp.maximum(top_m, unpacked(i, 4))
    weight = jnp.exp2(m_ref[0] - top_m)
    total = o_ref[0, 64:65, :] * weight
    mixed = o_ref[0, 0:64, :] * weight
    remote(orecv, orecv, o_s, o_r, up).wait_recv()
    for i in (2, 1, 0):
        weight = jnp.exp2(unpacked(i, 4) - top_m)
        total = total + unpacked(i, 0) * weight
        mixed = mixed + orecv[i].astype(F32) * weight
    mixed = mixed / total
    for k in range(NX):
        cols = mixed[:, 2 * QUARTER * k : 2 * QUARTER * (k + 1)]
        attended = jnp.concatenate([cols[:, 0:QUARTER], cols[:, QUARTER:]], axis=0).T.astype(BF16)
        for h in range(NC):
            asend[NC * k + h] = attended[OWN * h : OWN * (h + 1)]
    arecv[tp] = asend[tp]
    for d in range(1, NT):
        t, device = tp_peer(d)
        go(remote(asend.at[t], arecv.at[tp], a_s, a_r, device))
    loads[6].wait()
    arrived(arecv.at[pl.ds(0, NT - 1)], a_r)
    heads = jnp.concatenate([arecv[t] for t in range(NT)], axis=1)
    for i in range(4):
        cols = slice(512 * i, 512 * (i + 1))
        branch = jnp.dot(heads, wo[:, cols], preferred_element_type=F32)
        out[:, cols] = (
            lat[tp, :, cols].astype(F32) + vecs[2:3, cols] * branch
        ).astype(BF16)

    for ref, sem in (
        (mod1.at[pl.ds(0, NZ - 1)], mod1_s),
        (mod2.at[pl.ds(0, NY - 1)], mod2_s),
        (mod3.at[pl.ds(0, NT - 1)], mod3_s),
        (lat.at[pl.ds(0, NT - 1)], lat_s),
        (qraw.at[pl.ds(0, NY - 1)], q_s),
        (kv.at[pl.ds(0, NZ - 1)], kv_s),
        (ctx.at[0, pl.ds(0, NZ - 1)], ctx_s),
        (ctx.at[pl.ds(0, NY - 1)], cy_s),
        (qraw, o_s),
        (lmsend, lm_s),
        (arecv.at[pl.ds(0, NT - 1)], a_s),
    ):
        remote(ref, ref, sem, sem, up).wait_send()


def on_device(
    latent,
    context,
    condition,
    context_condition,
    norm_gain,
    shift_weight,
    scale_weight,
    gate_weight,
    query_weight,
    key_weight,
    value_weight,
    query_gain,
    key_gain,
    output_weight,
):
    hbm = pl.BlockSpec(memory_space=pl.ANY)
    dma, V = pltpu.SemaphoreType.DMA, pltpu.VMEM
    return pl.pallas_call(
        kernel,
        out_shape=pltpu.VMEM((OWN, D), BF16),
        in_specs=[hbm] * 14,
        out_specs=pl.BlockSpec(memory_space=pltpu.VMEM),
        scratch_shapes=[
            V((CTX, D), BF16),
            V((1, D), F32),
            V((1, D), F32),
            V((1, D), F32),
            V((1, HEAD), F32),
            V((1, HEAD), F32),
            V((128, 768), BF16),
            V((D, 256), BF16),
            V((128, D), BF16),
            V((1024, D), BF16),
            V((NZ, 8, 256), F32),
            V((NY, 8, 256), F32),
            V((NT, 8, 256), F32),
            V((8, D), F32),
            V((NT, OWN, D), BF16),
            V((NT, OWN, 128), F32),
            V((2 * QUARTER, D), BF16),
            V((4, 16, TOK), F32),
            V((NY, NX, HEAD, 2 * QUARTER), BF16),
            V((NY, 2 * HEAD, COLS), BF16),
            V((NZ, 512, 128), BF16),
            V((NZ + 1, TOK, 128), BF16),
            V((NZ + 1, 80, TOK), BF16),
            V((NY, NZ, CTX, 128), BF16),
            V((NY, 1, COLS), F32),
            V((NY, 80, COLS), F32),
            V((2, TOK, COLS), F32),
            V((2, 1, COLS), F32),
            V((NY - 1, HEAD, COLS), BF16),
            V((NY - 1, 8, 256), F32),
            V((NY - 1, HEAD, COLS), BF16),
            V((NY - 1, 8, 256), F32),
            V((2, HEAD // 2, COLS), BF16),
            V((NT, OWN, 128), BF16),
            V((NT, OWN, 128), BF16),
            dma((14,)),
            dma,
            dma,
            dma,
            dma,
            dma,
            dma,
            dma,
            dma((4,)),
            dma((4,)),
            dma((7,)),
            dma,
            dma((NY - 1,)),
            dma,
            dma((NZ - 1, NX)),
            dma,
            dma,
            dma,
            dma,
            dma,
            dma,
            dma((2,)),
            dma,
            dma,
            dma,
            dma,
        ],
        compiler_params=pltpu.CompilerParams(
            collective_id=0, has_side_effects=True, vmem_limit_bytes=60 * 2**20
        ),
    )(
        latent,
        context,
        condition.reshape(1, D),
        context_condition.reshape(1, D),
        norm_gain.reshape(1, D),
        shift_weight,
        scale_weight,
        gate_weight,
        query_weight,
        key_weight.T,
        value_weight.T,
        query_gain.reshape(1, HEAD),
        key_gain.reshape(1, HEAD),
        output_weight,
    )


def solution(mesh):
    split = Mesh(mesh.devices.reshape(NZ, NY, NX, NC), AXES)
    seq, tp, everything = ("z", "y"), ("x", "c"), AXES
    return jax.shard_map(
        on_device,
        mesh=split,
        in_specs=(
            P(everything, None),
            P(seq, None),
            P(),
            P(),
            P(),
            P(seq, tp),
            P(seq, tp),
            P(seq, tp),
            P(None, tp),
            P(None, tp),
            P(None, tp),
            P(),
            P(),
            P(),
        ),
        out_specs=P(everything, None),
        check_vma=False,
    )
```
